32 devices in a mesh: ep: 16 (over z, x, core), tp: 2 (over y).
Axes of the slice: x: 2, y: 2, z: 4, core: 2. Of those that a mesh axis runs over, the one named last changes fastest.
Arguments:
- tokens: bfloat16 [192, 1024], P('ep'), may hold values from -6 to 6
- norm_gain: float32 [1024], replicated, may hold values from 0.1 to 1.9
- w_query: bfloat16 [1024, 512], P(None, 'tp'), may hold values from -0.1875 to 0.1875
- w_key: bfloat16 [1024, 512], P(None, 'tp'), may hold values from -0.1875 to 0.1875
- w_value: bfloat16 [1024, 512], P(None, 'tp'), may hold values from -0.1875 to 0.1875
- w_input_gate: bfloat16 [1024, 4], replicated, may hold values from -0.1875 to 0.1875
- w_forget_gate: bfloat16 [1024, 4], replicated, may hold values from -0.1875 to 0.1875
- input_bias: float32 [4], replicated, may hold values from -2 to 1
- forget_bias: float32 [4], replicated, may hold values from 0 to 4
- state_c: float32 [192, 4, 128, 128], P('ep', 'tp'), may hold values from -1.75 to 1.75
- state_n: float32 [192, 4, 128], P('ep', 'tp'), may hold values from -1.75 to 1.75
- state_m: float32 [192, 4], P('ep', 'tp'), may hold values from -1 to 2
- w_mixer_out: bfloat16 [512, 1024], P('tp'), may hold values from -0.25 to 0.25
- ffn_gain: float32 [1024], replicated, may hold values from 0.1 to 1.9
- routes: int32 [192, 6], P('ep'), may hold values from 0 to 15, all different within a row; in each aligned block of 12 rows (0 to 11, 12 to 23, ...) at most 10 rows name the same one
- route_scale: bfloat16 [192, 6], P('ep'), may hold values from 0.099609375 to 1
- w_expert_gate: bfloat16 [16, 1024, 1024], P('ep', None, 'tp'), may hold values from -0.375 to 0.375
- w_expert_up: bfloat16 [16, 1024, 1024], P('ep', None, 'tp'), may hold values from -0.375 to 0.375
- w_expert_down: bfloat16 [16, 1024, 1024], P('ep', 'tp'), may hold values from -0.1875 to 0.1875
- w_dense_gate: bfloat16 [1024, 512], P(None, 'tp'), may hold values from -0.1875 to 0.1875
- w_dense_up: bfloat16 [1024, 512], P(None, 'tp'), may hold values from -0.1875 to 0.1875
- w_dense_down: bfloat16 [512, 1024], P('tp'), may hold values from -0.5 to 0.5
- w_branch_gate: bfloat16 [1024], replicated, may hold values from -0.1875 to 0.1875
Outputs:
- output: bfloat16 [192, 1024], P('ep', 'tp')
- new_c: float32 [192, 4, 128, 128], P('ep', 'tp')
- new_n: float32 [192, 4, 128], P('ep', 'tp')
- new_m: float32 [192, 4], P('ep', 'tp')
The draws below stay inside these ranges and needn't reach their ends.
Inputs may be any that keep to these rules, and one draw needn't show every extreme that they name: `routes`: each row names 6 different experts. Among the rows of one index of ep no expert is named by more than 10 rows, a bound that some block reaches of them.
All inputs are finite; a program needn't handle non-finite values.
Results may differ from the reference program's by a relative error of at most 0.018.
Values may be sent and summed in bfloat16 or wider, within the bound.
A program may use at most 64 MiB of HBM per device.

```python
import math
import jax
import jax.numpy as jnp
import numpy as np
from jax import lax

D = 1024
HEADS = 4
DQK = 128
DV = 128
D_EXPERT = 1024
DENSE_FF = 512
TOP_K = 6
SEQ_DEV = 12
EXPERTS = 16
TOKENS = 192
CAP = 10
N_TP = 2


def block_scale(rng, dims, split, low, top_value):
    gain = 1.0
    for dim, parts in split:
        draws = jax.random.uniform(jax.random.fold_in(jax.random.fold_in(rng, 6), dim), (parts,), jnp.float32, low / len(split), top_value / len(split))
        gain = gain * jnp.repeat(jnp.exp(draws), dims[dim] // parts).reshape((-1,) + (1,) * (len(dims) - 1 - dim))
    return gain


def assign_block(rng, own, number, rows, count, top, most, slope):
    sequence = jax.random.permutation(rng, count)
    crowded, common = shares(count, rows * top, most, slope, True), shares(count, rows * top, most, slope, False)
    places = jnp.arange(count)

    def named(sizes, turn):
        used = int((sizes > 0).sum())
        fixed = max(1, used // 4)
        moved = fixed + (places - fixed + turn * (used - fixed)) % max(1, count - fixed)
        return jnp.zeros((count,), jnp.int32).at[sequence[jnp.where(places < fixed, places, moved)]].set(jnp.asarray(sizes, jnp.int32))

    sizes = jnp.where(number % 4 == 0, named(crowded, number // 4), named(common, number - number // 4 - 1))
    mixed = jax.random.permutation(jax.random.fold_in(own, 3), count)
    donor, taker = mixed[0:count // 2 * 2:2], mixed[1:count // 2 * 2:2]
    room = jnp.minimum(sizes[donor] - 1, most - sizes[taker]) // 2
    room = jnp.where((donor == sequence[0]) | (taker == sequence[0]) | (sizes[taker] == 0), 0, jnp.maximum(room, 0))
    moved = jax.random.randint(jax.random.fold_in(own, 4), (count // 2,), 0, 1 << 20) % (room + 1)
    sizes = sizes.at[donor].add(-moved).at[taker].add(moved)
    members = jnp.searchsorted(jnp.cumsum(sizes), jnp.arange(rows * top), side="right").astype(jnp.int32)
    listing = members.reshape(top, rows).T
    listing = listing[jax.random.permutation(jax.random.fold_in(own, 1), rows)]
    turn = jax.random.randint(jax.random.fold_in(own, 2), (rows, 1), 0, top)
    return jnp.take_along_axis(listing, (jnp.arange(top)[None, :] + turn) % top, axis=1)


def shares(number_of, total, most, lean, full):
    weights = [(1 << 20) // math.isqrt(standing ** lean) + 1 for standing in range(1, number_of + 1)]
    largest = most if full else min(most, max(-(-total // number_of), total * weights[0] // sum(weights)))
    least = 1 if total - largest >= number_of - 1 else 0
    given, surplus = [largest] + [least] * (number_of - 1), total - largest - least * (number_of - 1)
    while surplus > 0:
        free = [i for i in range(1, number_of) if given[i] < largest] or [i for i in range(1, number_of) if given[i] < most]
        whole, left = sum([weights[i] for i in free]), surplus
        for i in free:
            extra = min(most - given[i], max(1, left * weights[i] // whole), surplus)
            given[i] = given[i] + extra
            surplus = surplus - extra
    return np.array(given)


def scatter_about(own_key, shape, spread, limit, pieces=(), kind=jnp.bfloat16):
    array = jax.random.normal(own_key, shape, jnp.float32) * spread
    if len(pieces) > 0:
        array = block_scale(own_key, shape, pieces, -0.22, 0.18) * array
    return jnp.clip(array, min=-limit, max=limit).astype(kind)


def setup_inputs(seed: int = 0) -> dict:
    key_list = jax.random.split(jax.random.key(seed), 24)
    tokens = scatter_about(key_list[0], (TOKENS, D), 1.0, 6.0, ((0, 16),))
    norm_gain = jnp.clip(1.0 + 0.18 * jax.random.normal(key_list[1], (D,), jnp.float32), 0.1, 1.9)
    w_query = scatter_about(key_list[2], (D, HEADS * DQK), D ** -0.5, 0.1875, ((1, 2),))
    w_key = scatter_about(key_list[3], (D, HEADS * DQK), D ** -0.5, 0.1875, ((1, 2),))
    w_value = scatter_about(key_list[4], (D, HEADS * DV), D ** -0.5, 0.1875, ((1, 2),))
    w_input_gate = scatter_about(key_list[5], (D, HEADS), D ** -0.5, 0.1875)
    w_forget_gate = scatter_about(key_list[6], (D, HEADS), D ** -0.5, 0.1875)
    input_bias = jnp.clip(jax.random.uniform(key_list[7], (HEADS,), jnp.float32, -2.0, 1.0), -2.0, 1.0)
    forget_bias = jnp.clip(jax.random.uniform(key_list[8], (HEADS,), jnp.float32, 0.0, 4.0), 0.0, 4.0)
    state_c = scatter_about(key_list[9], (TOKENS, HEADS, DQK, DV), 0.3, 1.75, ((0, 16), (1, 2)), jnp.float32)
    state_n = scatter_about(key_list[10], (TOKENS, HEADS, DQK), 0.3, 1.75, ((0, 16), (1, 2)), jnp.float32)
    state_m = jnp.clip(-1.0 + 3.0 * jax.random.uniform(key_list[11], (TOKENS, HEADS), jnp.float32) ** block_scale(key_list[11], (TOKENS, HEADS), ((0, 16), (1, 2)), -0.2, 0.2), -1.0, 2.0)
    w_mixer_out = scatter_about(key_list[12], (HEADS * DV, D), (HEADS * DV) ** -0.5, 0.25, ((0, 2),))
    ffn_gain = jnp.clip(1.0 + 0.18 * jax.random.normal(key_list[13], (D,), jnp.float32), 0.1, 1.9)
    routes_keys = jax.random.split(jax.random.fold_in(key_list[14], 1), TOKENS // SEQ_DEV)
    routes_turns = jax.random.permutation(jax.random.fold_in(key_list[14], 3), TOKENS // SEQ_DEV)
    routes = jax.vmap(lambda own, number: assign_block(jax.random.fold_in(key_list[14], 2), own, number, SEQ_DEV, EXPERTS, TOP_K, CAP, 2))(routes_keys, routes_turns).reshape((TOKENS, TOP_K))
    route_scale = jnp.clip(jnp.exp(math.log(1.0) - 2.306499 * jax.random.uniform(key_list[15], (TOKENS, TOP_K), jnp.float32) ** block_scale(key_list[15], (TOKENS, TOP_K), ((0, 16),), -0.2, 0.2)), 0.099609375, 1.0).astype(jnp.bfloat16)
    w_expert_gate = scatter_about(key_list[16], (EXPERTS, D, D_EXPERT), (2.0 * D ** -0.5), 0.375, ((0, 16), (2, 2)))
    w_expert_up = scatter_about(key_list[17], (EXPERTS, D, D_EXPERT), (2.0 * D ** -0.5), 0.375, ((0, 16), (2, 2)))
    w_expert_down = scatter_about(key_list[18], (EXPERTS, D_EXPERT, D), D_EXPERT ** -0.5, 0.1875, ((0, 16), (1, 2)))
    w_dense_gate = scatter_about(key_list[19], (D, DENSE_FF), D ** -0.5, 0.1875, ((1, 2),))
    w_dense_up = scatter_about(key_list[20], (D, DENSE_FF), D ** -0.5, 0.1875, ((1, 2),))
    w_dense_down = scatter_about(key_list[21], (DENSE_FF, D), (DENSE_FF // 4) ** -0.5, 0.5, ((0, 2),))
    w_branch_gate = scatter_about(key_list[22], (D,), D ** -0.5, 0.1875)
    return {"tokens": tokens, "norm_gain": norm_gain, "w_query": w_query, "w_key": w_key, "w_value": w_value, "w_input_gate": w_input_gate, "w_forget_gate": w_forget_gate, "input_bias": input_bias, "forget_bias": forget_bias, "state_c": state_c, "state_n": state_n, "state_m": state_m, "w_mixer_out": w_mixer_out, "ffn_gain": ffn_gain, "routes": routes, "route_scale": route_scale, "w_expert_gate": w_expert_gate, "w_expert_up": w_expert_up, "w_expert_down": w_expert_down, "w_dense_gate": w_dense_gate, "w_dense_up": w_dense_up, "w_dense_down": w_dense_down, "w_branch_gate": w_branch_gate}


EPSILON = 1e-06
CLAMP_LIMIT = 7.0
SWISH_ALPHA = 1.702

def stored(values):
    return lax.optimization_barrier(values.astype(jnp.bfloat16)).astype(jnp.float32)

def rms_scaled(values, gain_vec):
    values = values.astype(jnp.float32)
    scaled = values * lax.rsqrt(lax.optimization_barrier(jnp.mean(values * values, axis=-1, keepdims=True)) + EPSILON)
    return scaled * gain_vec.astype(jnp.float32)

def slot_tables(route_blocks, expert_ids, weight_blocks, capacity, top_count):
    entries = route_blocks.shape[1]
    matched = (route_blocks[:, None, :] == expert_ids[None, :, None]).astype(jnp.int32)
    ranking = jnp.cumsum(matched, axis=2, dtype=jnp.int32) - 1
    slot_ids = jnp.arange(capacity, dtype=jnp.int32)
    chosen = (matched[:, :, None, :] == 1) & (ranking[:, :, None, :] == slot_ids[None, None, :, None])
    slot_hot = jnp.where(chosen, 1.0, 0.0).astype(jnp.float32)
    entry_ids = jnp.arange(entries, dtype=jnp.int32)
    token_ids = jnp.arange(entries // top_count, dtype=jnp.int32)
    owner = jnp.where(entry_ids[:, None] // top_count == token_ids[None, :], 1.0, 0.0).astype(jnp.float32)
    token_hot = jnp.einsum('becj,js->becs', slot_hot, owner, precision=lax.Precision.HIGHEST)
    slot_weight = jnp.einsum('becj,bj->bec', slot_hot, weight_blocks, precision=lax.Precision.HIGHEST)
    return (token_hot, slot_weight)

def reference(tokens, norm_gain, w_query, w_key, w_value, w_input_gate, w_forget_gate, input_bias, forget_bias, state_c, state_n, state_m, w_mixer_out, ffn_gain, routes, route_scale, w_expert_gate, w_expert_up, w_expert_down, w_dense_gate, w_dense_up, w_dense_down, w_branch_gate):
    row_count = tokens.shape[0]
    normed = rms_scaled(tokens, norm_gain).astype(jnp.bfloat16)
    queries = stored(jnp.dot(normed, w_query, preferred_element_type=jnp.float32)).reshape(row_count, HEADS, DQK)
    key_rows = stored(jnp.dot(normed, w_key, preferred_element_type=jnp.float32)).reshape(row_count, HEADS, DQK)
    value_rows = stored(jnp.dot(normed, w_value, preferred_element_type=jnp.float32)).reshape(row_count, HEADS, DV)
    input_pre = jnp.dot(normed, w_input_gate, preferred_element_type=jnp.float32) + input_bias
    forget_log = jax.nn.log_sigmoid(jnp.dot(normed, w_forget_gate, preferred_element_type=jnp.float32) + forget_bias)
    new_m = jnp.maximum(forget_log + state_m, input_pre)
    forget_factor = jnp.exp(forget_log + state_m - new_m)
    input_factor = jnp.exp(input_pre - new_m)
    key_scaled = key_rows * DQK ** (-0.5)
    new_c = forget_factor[..., None, None] * state_c + input_factor[..., None, None] * (key_scaled[..., :, None] * value_rows[..., None, :])
    new_n = forget_factor[..., None] * state_n + input_factor[..., None] * key_scaled
    numer = jnp.einsum('thd,thdv->thv', queries, new_c, precision=lax.Precision.HIGHEST)
    denom = jnp.einsum('thd,thd->th', queries, new_n, precision=lax.Precision.HIGHEST)
    head_out = (numer / jnp.maximum(jnp.abs(denom), 1.0)[..., None]).astype(jnp.bfloat16).reshape(row_count, HEADS * DV)
    group_width = HEADS // N_TP * DV
    mixer_total = jnp.zeros((row_count, D), jnp.float32)
    for group in range(N_TP):
        lower = group * group_width
        mixer_total = mixer_total + stored(jnp.dot(head_out[:, lower:lower + group_width], w_mixer_out[lower:lower + group_width], preferred_element_type=jnp.float32))
    mixer_out = mixer_total.astype(jnp.bfloat16)
    residual = tokens.astype(jnp.float32) + mixer_out.astype(jnp.float32)
    ffn_in = rms_scaled(residual, ffn_gain).astype(jnp.bfloat16)
    scale_values = route_scale.astype(jnp.float32)
    route_weight = scale_values / lax.optimization_barrier(jnp.sum(scale_values, axis=1, keepdims=True))
    block_count = row_count // SEQ_DEV
    route_blocks = routes.reshape(block_count, SEQ_DEV * TOP_K)
    weight_blocks = route_weight.reshape(block_count, SEQ_DEV * TOP_K)
    token_blocks = ffn_in.astype(jnp.float32).reshape(block_count, SEQ_DEV, D)
    part_width = D_EXPERT // N_TP

    def one_expert(total, inputs):
        gate_weight, up_weight, down_weight, expert = inputs
        token_hot, slot_weight = slot_tables(route_blocks, expert[None], weight_blocks, CAP, TOP_K)
        token_hot = token_hot[:, 0]
        slot_weight = slot_weight[:, 0]
        slot_rows = jnp.einsum('bcs,bsd->bcd', token_hot, token_blocks, precision=lax.Precision.HIGHEST).astype(jnp.bfloat16).reshape(block_count * CAP, D)
        gate_pre = jnp.minimum(jnp.dot(slot_rows, gate_weight, preferred_element_type=jnp.float32), CLAMP_LIMIT)
        up_pre = jnp.clip(jnp.dot(slot_rows, up_weight, preferred_element_type=jnp.float32), -CLAMP_LIMIT, CLAMP_LIMIT)
        hidden = (gate_pre * jax.nn.sigmoid(SWISH_ALPHA * gate_pre) * (up_pre + 1.0)).astype(jnp.bfloat16)
        expert_out = jnp.zeros((block_count * CAP, D), jnp.float32)
        for part in range(N_TP):
            lower = part * part_width
            expert_out = expert_out + stored(jnp.dot(hidden[:, lower:lower + part_width], down_weight[lower:lower + part_width], preferred_element_type=jnp.float32))
        weighted = expert_out.reshape(block_count, CAP, D) * slot_weight[..., None]
        total = total + jnp.einsum('bcs,bcd->bsd', token_hot, weighted, precision=lax.Precision.HIGHEST)
        return (total, None)
    moe, _ = lax.scan(one_expert, jnp.zeros((block_count, SEQ_DEV, D), jnp.float32), (w_expert_gate, w_expert_up, w_expert_down, jnp.arange(EXPERTS, dtype=jnp.int32)))
    dense_gate_pre = jnp.dot(ffn_in, w_dense_gate, preferred_element_type=jnp.float32)
    dense_hidden = (jax.nn.silu(dense_gate_pre) * jnp.dot(ffn_in, w_dense_up, preferred_element_type=jnp.float32)).astype(jnp.bfloat16)
    dense = jnp.dot(dense_hidden, w_dense_down, preferred_element_type=jnp.float32)
    branch_weight = jax.nn.sigmoid(jnp.dot(ffn_in, w_branch_gate, preferred_element_type=jnp.float32))
    output = (residual + moe.reshape(row_count, D) + branch_weight[:, None] * dense).astype(jnp.bfloat16)
    return (output, new_c, new_n, new_m)
```

```python
import functools

import jax
import jax.numpy as jnp
from jax import lax
from jax.experimental import pallas as pl
from jax.experimental.pallas import tpu as pltpu
from jax.sharding import PartitionSpec as P

EPSILON = 1e-06
CLAMP_LIMIT = 7.0
SWISH_ALPHA = 1.702
MESH = pl.DeviceIdType.MESH
F32 = jnp.float32
BF16 = jnp.bfloat16
VMEM_LIMIT = 60000 * 1024
scope = jax.named_scope


def padded(values, rows):
    extra = rows - values.shape[0]
    if extra == 0:
        return values
    return jnp.concatenate([values, jnp.zeros((extra, values.shape[1]), values.dtype)], axis=0)


def dot(left, right):
    return jnp.dot(left, right, preferred_element_type=F32)


def dot_nt(left, right):
    return lax.dot_general(left, right, (((1,), (1,)), ((), ())), preferred_element_type=F32)


def rms_scaled(values, gain):
    scale = lax.rsqrt(jnp.mean(values * values, axis=-1, keepdims=True) + EPSILON)
    return values * scale * gain


def to_column(row, rows):
    shape = (rows, row.shape[1])
    same = lax.broadcasted_iota(jnp.int32, shape, 0) == lax.broadcasted_iota(jnp.int32, shape, 1)
    return jnp.sum(jnp.where(same, row, 0.0), axis=1, keepdims=True)


def to_row(col, lanes):
    shape = (col.shape[0], lanes)
    same = lax.broadcasted_iota(jnp.int32, shape, 0) == lax.broadcasted_iota(jnp.int32, shape, 1)
    return jnp.sum(jnp.where(same, col, 0.0), axis=0, keepdims=True)


def column(values, index):
    lanes = lax.broadcasted_iota(jnp.int32, values.shape, 1)
    return jnp.sum(jnp.where(lanes == index, values, 0.0), axis=1, keepdims=True)


def dense_rows(rows):
    return 8 < rows <= 12


def block_shape(rows, pad_rows, width):
    return (8, width + width // 2) if dense_rows(rows) else (pad_rows, width)


def pack(values, rows):
    if not dense_rows(rows):
        return values
    half = values.shape[1] // 2
    low, high = values[8:16, :half], values[8:16, half:]
    top = lax.broadcasted_iota(jnp.int32, low.shape, 0) < 4
    return jnp.concatenate([values[:8], jnp.where(top, low, pltpu.roll(high, 4, 0))], axis=1)


def unpack(block, rows):
    if not dense_rows(rows):
        return block
    width = block.shape[1] // 3 * 2
    tail = block[:, width:]
    return jnp.concatenate(
        [block[:, :width], jnp.concatenate([tail, pltpu.roll(tail, 4, 0)], axis=1)], axis=0
    )


def partner(index, step, size, sign):
    if size & (size - 1):
        return lax.rem(index + sign * step + size, size)
    bit = 1
    while bit < size:
        if step & bit:
            index = index + bit * (1 - 2 * lax.rem(lax.div(index, bit), 2))
        bit *= 2
    return index


def layer_kernel(
    sizes,
    tokens_hbm,
    gain_hbm,
    wi_hbm,
    wf_hbm,
    ib_hbm,
    fb_hbm,
    m_hbm,
    n_hbm,
    wq_hbm,
    wk_hbm,
    wv_hbm,
    c_hbm,
    mix_hbm,
    fgain_hbm,
    routes_hbm,
    scale_hbm,
    wb_hbm,
    dg_hbm,
    du_hbm,
    dd_hbm,
    eg_hbm,
    eu_hbm,
    ed_hbm,
    out_ref,
    newc_ref,
    newn_ref,
    newm_ref,
    tokens_ref,
    gain_ref,
    wi_ref,
    wf_ref,
    ib_ref,
    fb_ref,
    m_ref,
    n_ref,
    wq_ref,
    wk_ref,
    wv_ref,
    c_buf,
    mix_buf,
    fgain_ref,
    routes_ref,
    scale_ref,
    wb_ref,
    dg,
    du,
    dd,
    eg,
    eu,
    ed,
    part_send,
    mixed,
    own_w,
    weights,
    block_send,
    blocks,
    inputs_ref,
    ret_send,
    ret,
    load_sem,
    c_sem,
    mix_s,
    mix_r,
    w_s,
    w_r,
    g_s,
    g_r,
    e_s,
    e_r,
    r_s,
    r_r,
):
    nz, nx, nc, ntp = sizes
    ep = lax.axis_index("ep")
    tp = lax.axis_index("tp")
    c = lax.rem(ep, nc)
    x = lax.rem(lax.div(ep, nc), nx)
    z = lax.div(ep, nc * nx)
    rows, width = tokens_ref.shape
    pad_rows = inputs_ref.shape[0] // (nz * nx)
    heads = m_ref.shape[0]
    dk, dv = c_buf.shape[2], c_buf.shape[3]
    cw = width // ntp
    first = tp * heads

    def place(dz, dx, sign):
        return partner(z, dz, nz, sign) * nx + partner(x, dx, nx, sign)

    def plane(dy, sign):
        return partner(tp, dy, ntp, sign)

    def at(dz, dx, dy, sign):
        return {"ep": place(dz, dx, sign) * nc + c, "tp": plane(dy, sign)}

    def core_at(dc):
        return {"ep": ep - c + lax.rem(c + dc, nc)}

    def remote(src, dst, send, recv, device):
        return pltpu.make_async_remote_copy(
            src_ref=src, dst_ref=dst, send_sem=send, recv_sem=recv, device_id=device, device_id_type=MESH
        )

    pending = []

    def send(copy):
        copy.start()
        pending.append(copy)

    places = [(dz, dx) for dz in range(nz - 1, -1, -1) for dx in range(nx - 1, -1, -1)]
    other_places = places[:-1]
    other_planes = list(range(1, ntp))

    barrier = pltpu.get_barrier_semaphore()
    count = 0
    for dz, dx in places:
        for dy in range(ntp):
            if (dz, dx, dy) != (0, 0, 0):
                pl.semaphore_signal(barrier, inc=1, device_id=at(dz, dx, dy, 1), device_id_type=MESH)
                count += 1
    for dc in range(1, nc):
        pl.semaphore_signal(barrier, inc=1, device_id=core_at(dc), device_id_type=MESH)
        count += 1

    loads = [
        pltpu.make_async_copy(src, dst, load_sem.at[i])
        for i, (src, dst) in enumerate(
            (
                (tokens_hbm, tokens_ref),
                (gain_hbm, gain_ref),
                (wi_hbm, wi_ref),
                (wf_hbm, wf_ref),
                (ib_hbm, ib_ref),
                (fb_hbm, fb_ref),
                (m_hbm, m_ref),
                (n_hbm, n_ref),
                (wq_hbm, wq_ref),
                (wk_hbm, wk_ref),
                (wv_hbm, wv_ref),
                (mix_hbm, mix_buf),
                (routes_hbm, routes_ref),
                (scale_hbm, scale_ref),
                (fgain_hbm, fgain_ref),
                (wb_hbm, wb_ref),
                (dg_hbm, dg),
                (du_hbm, du),
                (dd_hbm, dd),
                (eg_hbm.at[0], eg.at[0]),
                (eu_hbm.at[0], eu.at[0]),
                (ed_hbm.at[0], ed.at[0]),
            )
        )
    ]

    def c_load(t):
        return pltpu.make_async_copy(c_hbm.at[t], c_buf.at[t], c_sem.at[t])

    for load in loads[:11]:
        load.start()
    for t in range(rows):
        c_load(t).start()
    for load in loads[11:16]:
        load.start()

    with scope("norm"):
        for load in loads[:2]:
            load.wait()
        tokens = padded(tokens_ref[...].astype(F32), pad_rows)
        normed = rms_scaled(tokens, gain_ref[...]).astype(BF16)
    with scope("gates"):
        for load in loads[2:8]:
            load.wait()
        pre_all = dot_nt(normed, wi_ref[...]) + ib_ref[...]
        fg_all = dot_nt(normed, wf_ref[...]) + fb_ref[...]
        fg_all = jnp.minimum(fg_all, 0.0) - jnp.log(1.0 + jnp.exp(-jnp.abs(fg_all)))
    with scope("qkv"):
        for load in loads[8:11]:
            load.wait()
        queries = dot(normed, wq_ref[...]).astype(BF16)
        keys = dot(normed, wk_ref[...]).astype(BF16).astype(F32)
        values = dot(normed, wv_ref[...]).astype(BF16).astype(F32)
    key_scale = dk**-0.5
    row_ids = lax.broadcasted_iota(jnp.int32, (pad_rows, dk), 0)
    per_head = []
    with scope("heads"):
        for h in range(heads):
            pre = column(pre_all, first + h)
            shifted = column(fg_all, first + h) + to_column(m_ref[h : h + 1, :], pad_rows)
            new_m = jnp.maximum(shifted, pre)
            forget = jnp.exp(shifted - new_m)
            inflow = jnp.exp(pre - new_m)
            newm_ref[h : h + 1, :] = to_row(new_m, rows)
            q = queries[:, h * dk : (h + 1) * dk].astype(F32)
            k = keys[:, h * dk : (h + 1) * dk] * (inflow * key_scale)
            v = values[:, h * dv : (h + 1) * dv]
            new_n = forget * padded(n_ref[:, h, :], pad_rows) + k
            newn_ref[:, h, :] = new_n[:rows]
            denom = jnp.maximum(jnp.abs(jnp.sum(q * new_n, axis=1, keepdims=True)), 1.0)
            inner = jnp.sum(q * k, axis=1, keepdims=True)
            wide_q = jnp.concatenate([jnp.where(row_ids == t, q, 0.0) for t in range(rows)], axis=1)
            per_head.append((forget, k, v, denom, inner, wide_q.astype(BF16)))
    with scope("readout"):
        for t in range(rows):
            c_load(t).wait()
        outs = []
        for h in range(heads):
            forget, _, v, denom, inner, wide_q = per_head[h]
            memory = c_buf[:, h].reshape(rows * dk, dv).astype(BF16)
            outs.append((forget * dot(wide_q, memory) + inner * v) / denom)
        head_out = jnp.concatenate(outs, axis=1).astype(BF16)
    with scope("mix"):
        loads[11].wait()
        part = dot(head_out, mix_buf[...]).astype(BF16).astype(F32)
        part_send[...] = pack(part, rows).astype(BF16)
    for load in loads[16:]:
        load.start()
    with scope("barrier"):
        pl.semaphore_wait(barrier, count)

    def mix_copy(dy):
        return remote(part_send, mixed.at[dy - 1], mix_s.at[dy - 1], mix_r.at[dy - 1], at(0, 0, dy, 1))

    for dy in other_planes:
        send(mix_copy(dy))

    def expert_copies(dc):
        return [
            remote(src.at[0], dst.at[dc], e_s.at[dc, i], e_r.at[dc, i], core_at(dc))
            for i, (src, dst) in enumerate(((eg_hbm, eg), (eu_hbm, eu), (ed_hbm, ed)))
        ]

    for dc in range(1, nc):
        for copy in expert_copies(dc):
            send(copy)

    with scope("routes"):
        for load in loads[12:14]:
            load.wait()
        scale = scale_ref[...].astype(F32)
        route_weight = scale / jnp.sum(scale, axis=0, keepdims=True)
        experts = own_w.shape[0] * nc
        ids = lax.broadcasted_iota(jnp.int32, (experts, rows), 0)
        table = jnp.zeros((experts, rows), F32)
        for k in range(routes_ref.shape[0]):
            table = table + jnp.where(ids == routes_ref[k : k + 1, :], route_weight[k : k + 1, :], 0.0)
        table = jnp.concatenate([table, jnp.zeros((experts, own_w.shape[2] - rows), F32)], axis=1)
        for e in range(experts):
            own_w[e // nc, e % nc : e % nc + 1, :] = table[e : e + 1, :]

        def w_copy(dz, dx):
            return remote(
                own_w.at[place(dz, dx, 1)],
                weights.at[dz, dx],
                w_s.at[dz, dx],
                w_r.at[dz, dx],
                at(dz, dx, 0, 1),
            )

        for dz, dx in other_places:
            send(w_copy(dz, dx))
        weights[0, 0] = own_w[place(0, 0, 1)]

    with scope("ywait"):
        total = part
        for dy in other_planes:
            mix_copy(dy).wait_recv()
            total = total + unpack(mixed[dy - 1].astype(F32), rows)
    with scope("norm2"):
        loads[14].wait()
        residual = tokens + total.astype(BF16).astype(F32)
        ffn_f32 = rms_scaled(residual, fgain_ref[...])
        ffn_in = ffn_f32.astype(BF16)
        block_send[...] = pack(ffn_in.astype(F32), rows).astype(BF16)
        inputs_ref[:pad_rows] = ffn_in

    def g_copy(dz, dx):
        return remote(block_send, blocks.at[dz, dx], g_s.at[dz, dx], g_r.at[dz, dx], at(dz, dx, 0, 1))

    for dz, dx in other_places:
        send(g_copy(dz, dx))

    with scope("dense"):
        for load in loads[15:19]:
            load.wait()
        dense_hidden = (jax.nn.silu(dot(ffn_in, dg[...])) * dot(ffn_in, du[...])).astype(BF16)
        wb = wb_ref[...].astype(F32)
        lanes = wb.shape[1]
        wide = ffn_in.astype(F32)
        branch = jnp.zeros((pad_rows, lanes), F32)
        for i in range(wb.shape[0]):
            branch = branch + wide[:, i * lanes : (i + 1) * lanes] * wb[i : i + 1, :]
        branch = jax.nn.sigmoid(jnp.sum(branch, axis=1, keepdims=True))

        def dense_part(dy):
            cols = pl.ds(pl.multiple_of(plane(dy, -1) * cw, cw), cw)
            return dot(dense_hidden, dd[:, cols]) * branch

        dense = [dense_part(dy) for dy in range(ntp)]
        own = dense[0]
        for j in range(ntp):
            own = own + jnp.where(tp == j, residual[:, j * cw : (j + 1) * cw], 0.0)

    with scope("newc"):
        for h in range(heads):
            forget, k, v, _, _, _ = per_head[h]
            k_t = k.T
            for t in range(rows):
                newc_ref[t, h] = forget[t : t + 1] * c_buf[t, h] + k_t[:, t : t + 1] * v[t : t + 1]

    with scope("factor"):
        for dz, dx in other_places:
            w_copy(dz, dx).wait_recv()
        factors = []
        for dc in range(nc):
            core = lax.rem(c + dc, nc)
            factors.append(
                jnp.concatenate(
                    [
                        to_column(weights[dz, dx, pl.ds(core, 1), :], pad_rows)
                        for dz in range(nz)
                        for dx in range(nx)
                    ],
                    axis=0,
                )
            )
    with scope("gwait"):
        for dz, dx in other_places[::-1]:
            g_copy(dz, dx).wait_recv()
            at_row = (dz * nx + dx) * pad_rows
            inputs_ref[at_row : at_row + pad_rows] = unpack(blocks[dz, dx].astype(F32), rows).astype(BF16)
    hidden = []
    for dc in range(nc):
        with scope("wwait"):
            if dc == 0:
                for load in loads[19:]:
                    load.wait()
            else:
                for copy in expert_copies(dc):
                    copy.wait_recv()
        with scope("expert"):
            inputs = inputs_ref[...]
            gate = jnp.minimum(dot(inputs, eg[dc]), CLAMP_LIMIT)
            up = jnp.clip(dot(inputs, eu[dc]), -CLAMP_LIMIT, CLAMP_LIMIT)
            act = gate * jax.nn.sigmoid(SWISH_ALPHA * gate) * (up + 1.0)
            hidden.append((act * factors[dc]).astype(BF16))

    def r_copy(dz, dx, dy):
        return remote(
            ret_send.at[dy, dz, dx],
            ret.at[dy, dz, dx],
            r_s.at[dy, dz, dx],
            r_r.at[dy, dz, dx],
            at(dz, dx, dy, -1),
        )

    for dy in other_planes[::-1] + [0]:
        with scope("down"):
            cols = pl.ds(pl.multiple_of(plane(dy, -1) * cw, cw), cw)
            result = dot(hidden[0], ed[0, :, cols])
            for dc in range(1, nc):
                result = result + dot(hidden[dc], ed[dc, :, cols])
            for dz, dx in places:
                at_row = (dz * nx + dx) * pad_rows
                value = result[at_row : at_row + pad_rows]
                if (dz, dx, dy) == (0, 0, 0):
                    own = own + value
                    continue
                if (dz, dx) == (0, 0):
                    value = value + dense[dy]
                ret_send[dy, dz, dx] = pack(value, rows).astype(BF16)
                send(r_copy(dz, dx, dy))

    with scope("final"):
        total = None
        for dy in range(ntp):
            for dz, dx in places[::-1]:
                if (dz, dx, dy) == (0, 0, 0):
                    continue
                r_copy(dz, dx, dy).wait_recv()
                value = ret[dy, dz, dx].astype(F32)
                total = value if total is None else total + value
        if total is not None:
            own = own + unpack(total, rows)
        out_ref[...] = own[:rows].astype(BF16)
    with scope("sendwait"):
        for copy in pending:
            copy.wait_send()


def store_kernel(out_v, c_v, n_v, m_v, out_h, c_h, n_h, m_h, sem, c_sem):
    copies = [
        pltpu.make_async_copy(src, dst, sem.at[i])
        for i, (src, dst) in enumerate(((out_v, out_h), (n_v, n_h), (m_v, m_h)))
    ]
    copies += [pltpu.make_async_copy(c_v.at[t], c_h.at[t], c_sem.at[t]) for t in range(c_v.shape[0])]
    for copy in copies:
        copy.start()
    for copy in copies:
        copy.wait()


def local(
    sizes,
    tokens,
    norm_gain,
    w_query,
    w_key,
    w_value,
    w_input_gate,
    w_forget_gate,
    input_bias,
    forget_bias,
    state_c,
    state_n,
    state_m,
    w_mixer_out,
    ffn_gain,
    routes,
    route_scale,
    w_expert_gate,
    w_expert_up,
    w_expert_down,
    w_dense_gate,
    w_dense_up,
    w_dense_down,
    w_branch_gate,
):
    nz, nx, nc, ntp = sizes
    rows, width = tokens.shape
    pad_rows = -(-rows // 16) * 16
    cw = width // ntp
    vmem = pl.BlockSpec(memory_space=pltpu.VMEM)
    hbm = pl.BlockSpec(memory_space=pl.ANY)
    dma = pltpu.SemaphoreType.DMA
    wide_block = block_shape(rows, pad_rows, width)
    slim_block = block_shape(rows, pad_rows, cw)
    planes = max(1, ntp - 1)
    outs = pl.pallas_call(
        functools.partial(layer_kernel, sizes),
        name="layer",
        out_shape=(
            pltpu.VMEM((rows, cw), BF16),
            pltpu.VMEM(state_c.shape, F32),
            pltpu.VMEM(state_n.shape, F32),
            pltpu.VMEM(state_m.shape[::-1], F32),
        ),
        in_specs=[hbm] * 23,
        out_specs=(vmem,) * 4,
        scratch_shapes=[
            pltpu.VMEM(tokens.shape, BF16),
            pltpu.VMEM((1, width), F32),
            pltpu.VMEM(w_input_gate.shape[::-1], BF16),
            pltpu.VMEM(w_forget_gate.shape[::-1], BF16),
            pltpu.VMEM((1, input_bias.shape[0]), F32),
            pltpu.VMEM((1, forget_bias.shape[0]), F32),
            pltpu.VMEM(state_m.shape[::-1], F32),
            pltpu.VMEM(state_n.shape, F32),
            pltpu.VMEM(w_query.shape, BF16),
            pltpu.VMEM(w_key.shape, BF16),
            pltpu.VMEM(w_value.shape, BF16),
            pltpu.VMEM(state_c.shape, F32),
            pltpu.VMEM(w_mixer_out.shape, BF16),
            pltpu.VMEM((1, width), F32),
            pltpu.VMEM(routes.shape[::-1], jnp.int32),
            pltpu.VMEM(route_scale.shape[::-1], BF16),
            pltpu.VMEM((width // 128, 128), BF16),
            pltpu.VMEM(w_dense_gate.shape, BF16),
            pltpu.VMEM(w_dense_up.shape, BF16),
            pltpu.VMEM(w_dense_down.shape, BF16),
            pltpu.VMEM((nc,) + w_expert_gate.shape[1:], BF16),
            pltpu.VMEM((nc,) + w_expert_up.shape[1:], BF16),
            pltpu.VMEM((nc,) + w_expert_down.shape[1:], BF16),
            pltpu.VMEM(wide_block, BF16),
            pltpu.VMEM((planes,) + wide_block, BF16),
            pltpu.VMEM((nz * nx, nc, 128), F32),
            pltpu.VMEM((nz, nx, nc, 128), F32),
            pltpu.VMEM(wide_block, BF16),
            pltpu.VMEM((nz, nx) + wide_block, BF16),
            pltpu.VMEM((nz * nx * pad_rows, width), BF16),
            pltpu.VMEM((ntp, nz, nx) + slim_block, BF16),
            pltpu.VMEM((ntp, nz, nx) + slim_block, BF16),
            dma((22,)),
            dma((rows,)),
            dma((planes,)),
            dma((planes,)),
            dma((nz, nx)),
            dma((nz, nx)),
            dma((nz, nx)),
            dma((nz, nx)),
            dma((nc, 3)),
            dma((nc, 3)),
            dma((ntp, nz, nx)),
            dma((ntp, nz, nx)),
        ],
        compiler_params=pltpu.CompilerParams(
            vmem_limit_bytes=VMEM_LIMIT, collective_id=0, has_side_effects=True
        ),
    )(
        tokens,
        norm_gain.reshape(1, width),
        w_input_gate.T,
        w_forget_gate.T,
        input_bias.reshape(1, -1),
        forget_bias.reshape(1, -1),
        state_m.T,
        state_n,
        w_query,
        w_key,
        w_value,
        state_c,
        w_mixer_out,
        ffn_gain.reshape(1, width),
        routes.T,
        route_scale.T,
        w_branch_gate.reshape(width // 128, 128),
        w_dense_gate,
        w_dense_up,
        w_dense_down,
        w_expert_gate,
        w_expert_up,
        w_expert_down,
    )
    output, new_c, new_n, new_m = pl.pallas_call(
        store_kernel,
        name="store",
        out_shape=(
            jax.ShapeDtypeStruct((rows, cw), BF16),
            jax.ShapeDtypeStruct(state_c.shape, F32),
            jax.ShapeDtypeStruct(state_n.shape, F32),
            jax.ShapeDtypeStruct(state_m.shape[::-1], F32),
        ),
        in_specs=[vmem] * 4,
        out_specs=(hbm,) * 4,
        scratch_shapes=[dma((3,)), dma((rows,))],
        compiler_params=pltpu.CompilerParams(vmem_limit_bytes=1024 * 1024),
    )(*outs)
    return (output, new_c, new_n, new_m.T)


def solution(mesh):
    n_ep, n_tp = mesh.shape["ep"], mesh.shape["tp"]
    n_core = 2 if n_ep % 2 == 0 else 1
    n_x = n_tp if n_ep % (n_core * n_tp) == 0 else 1
    sizes = (n_ep // (n_core * n_x), n_x, n_core, n_tp)
    in_specs = (
        P("ep", None),
        P(),
        P(None, "tp"),
        P(None, "tp"),
        P(None, "tp"),
        P(),
        P(),
        P(),
        P(),
        P("ep", "tp", None, None),
        P("ep", "tp", None),
        P("ep", "tp"),
        P("tp", None),
        P(),
        P("ep", None),
        P("ep", None),
        P("ep", None, "tp"),
        P("ep", None, "tp"),
        P("ep", "tp", None),
        P(None, "tp"),
        P(None, "tp"),
        P("tp", None),
        P(),
    )
    out_specs = (P("ep", "tp"), P("ep", "tp", None, None), P("ep", "tp", None), P("ep", "tp"))
    return jax.shard_map(
        functools.partial(local, sizes),
        mesh=mesh,
        in_specs=in_specs,
        out_specs=out_specs,
        check_vma=False,
    )
```

```python
import functools

import jax
import jax.numpy as jnp
from jax import lax
from jax.experimental import pallas as pl
from jax.experimental.pallas import tpu as pltpu
from jax.sharding import PartitionSpec as P

EPSILON = 1e-06
CLAMP_LIMIT = 7.0
SWISH_ALPHA = 1.702
MESH = pl.DeviceIdType.MESH
F32 = jnp.float32
BF16 = jnp.bfloat16
VMEM_LIMIT = 60000 * 1024
scope = jax.named_scope


def padded(values, rows):
    extra = rows - values.shape[0]
    if extra == 0:
        return values
    return jnp.concatenate([values, jnp.zeros((extra, values.shape[1]), values.dtype)], axis=0)


def dot(left, right):
    return jnp.dot(left, right, preferred_element_type=F32)


def dot_nt(left, right):
    return lax.dot_general(left, right, (((1,), (1,)), ((), ())), preferred_element_type=F32)


def rms_scaled(values, gain):
    scale = lax.rsqrt(jnp.mean(values * values, axis=-1, keepdims=True) + EPSILON)
    return values * scale * gain


def to_column(row, rows):
    shape = (rows, row.shape[1])
    same = lax.broadcasted_iota(jnp.int32, shape, 0) == lax.broadcasted_iota(jnp.int32, shape, 1)
    return jnp.sum(jnp.where(same, row, 0.0), axis=1, keepdims=True)


def to_row(col, lanes):
    shape = (col.shape[0], lanes)
    same = lax.broadcasted_iota(jnp.int32, shape, 0) == lax.broadcasted_iota(jnp.int32, shape, 1)
    return jnp.sum(jnp.where(same, col, 0.0), axis=0, keepdims=True)


def column(values, index):
    lanes = lax.broadcasted_iota(jnp.int32, values.shape, 1)
    return jnp.sum(jnp.where(lanes == index, values, 0.0), axis=1, keepdims=True)


def dense_rows(rows):
    return 8 < rows <= 12


def block_shape(rows, pad_rows, width):
    return (8, width + width // 2) if dense_rows(rows) else (pad_rows, width)


def pack(values, rows):
    if not dense_rows(rows):
        return values
    half = values.shape[1] // 2
    low, high = values[8:16, :half], values[8:16, half:]
    top = lax.broadcasted_iota(jnp.int32, low.shape, 0) < 4
    return jnp.concatenate([values[:8], jnp.where(top, low, pltpu.roll(high, 4, 0))], axis=1)


def unpack(block, rows):
    if not dense_rows(rows):
        return block
    width = block.shape[1] // 3 * 2
    tail = block[:, width:]
    return jnp.concatenate(
        [block[:, :width], jnp.concatenate([tail, pltpu.roll(tail, 4, 0)], axis=1)], axis=0
    )


def partner(index, step, size, sign):
    if size & (size - 1):
        return lax.rem(index + sign * step + size, size)
    bit = 1
    while bit < size:
        if step & bit:
            index = index + bit * (1 - 2 * lax.rem(lax.div(index, bit), 2))
        bit *= 2
    return index


def step_between(a, b, size):
    if size & (size - 1):
        return lax.rem(b - a + size, size)
    step, bit = 0, 1
    while bit < size:
        step = step + bit * lax.rem(lax.div(a, bit) + lax.div(b, bit), 2)
        bit *= 2
    return step


def layer_kernel(
    sizes,
    tokens_hbm,
    gain_hbm,
    wi_hbm,
    wf_hbm,
    ib_hbm,
    fb_hbm,
    m_hbm,
    n_hbm,
    wq_hbm,
    wk_hbm,
    wv_hbm,
    c_hbm,
    mix_hbm,
    fgain_hbm,
    routes_hbm,
    scale_hbm,
    wb_hbm,
    dg_hbm,
    du_hbm,
    dd_hbm,
    eg_hbm,
    eu_hbm,
    ed_hbm,
    out_ref,
    newc_ref,
    newn_ref,
    newm_ref,
    tokens_ref,
    gain_ref,
    wi_ref,
    wf_ref,
    ib_ref,
    fb_ref,
    m_ref,
    n_ref,
    wq_ref,
    wk_ref,
    wv_ref,
    c_buf,
    mix_buf,
    fgain_ref,
    routes_ref,
    scale_ref,
    wb_ref,
    dg,
    du,
    dd,
    eg,
    eu,
    ed,
    part_send,
    mixed,
    own_w,
    weights,
    block_send,
    blocks,
    inputs_ref,
    ret_send,
    ret,
    load_sem,
    mix_s,
    mix_r,
    w_s,
    w_r,
    g_s,
    g_r,
    e_s,
    e_r,
    r_s,
    r_r,
):
    nz, nx, nc, ntp = sizes
    ep = lax.axis_index("ep")
    tp = lax.axis_index("tp")
    c = lax.rem(ep, nc)
    x = lax.rem(lax.div(ep, nc), nx)
    z = lax.div(ep, nc * nx)
    rows, width = tokens_ref.shape
    pad_rows = inputs_ref.shape[0] // (nz * nx)
    heads = m_ref.shape[0]
    dk, dv = c_buf.shape[2], c_buf.shape[3]
    cw = width // ntp
    first = tp * heads

    def place(dz, dx, sign):
        return partner(z, dz, nz, sign) * nx + partner(x, dx, nx, sign)

    def plane(dy, sign):
        return partner(tp, dy, ntp, sign)

    def at(dz, dx, dy, sign):
        return at_place(place(dz, dx, sign), dy, sign)

    def at_place(there, dy, sign):
        return {"ep": there * nc + c, "tp": plane(dy, sign)}

    def core_at(dc):
        return {"ep": ep - c + lax.rem(c + dc, nc)}

    def remote(src, dst, send, recv, device):
        return pltpu.make_async_remote_copy(
            src_ref=src, dst_ref=dst, send_sem=send, recv_sem=recv, device_id=device, device_id_type=MESH
        )

    def slot(dz, dx, dy=0):
        return (dy * nz + dz) * nx + dx - 1

    pending = []

    def send(copy):
        copy.start()
        pending.append(copy)

    def whole(sent, received, send_sem, recv_sem):
        return remote(sent, received, send_sem, recv_sem, far)

    far = at(nz - 1, nx - 1, 0, 1) if nz * nx > 1 else at(0, 0, ntp - 1, 1)
    def far_first(sign):
        upper = lax.div(2 * z, nz)
        steps = [(0, dx, place(0, dx, sign)) for dx in range(1, nx)]
        for i in range(nz - 1):
            down = nz - 1 - i - lax.div(i + z + 1, nz)
            up = i + 1 - lax.div(nz - 1 - i + z, nz)
            there = upper * up + (1 - upper) * down
            dz = step_between(z, there, nz) if sign > 0 else step_between(there, z, nz)
            for dx in range(nx - 1, -1, -1):
                steps.append((dz, dx, there * nx + partner(x, dx, nx, sign)))
        return steps

    places = [(dz, dx) for dz in range(nz - 1, -1, -1) for dx in range(nx - 1, -1, -1)]
    other_places = places[:-1]
    other_planes = list(range(1, ntp))

    def greet():
        barrier = pltpu.get_barrier_semaphore()
        near = [at(0, 0, dy, 1) for dy in other_planes] + [core_at(dc) for dc in range(1, nc)]
        near += [at(dz, dx, 0, 1) for dz, dx in other_places]
        for device in near:
            pl.semaphore_signal(barrier, inc=1, device_id=device, device_id_type=MESH)
        return barrier, len(near)

    def group(index, *pairs):
        return [pltpu.make_async_copy(src, dst, load_sem.at[index]) for src, dst in pairs]

    first_loads = group(0, (tokens_hbm, tokens_ref), (gain_hbm, gain_ref))
    gate_loads = group(
        1,
        (wi_hbm, wi_ref),
        (wf_hbm, wf_ref),
        (ib_hbm, ib_ref),
        (fb_hbm, fb_ref),
        (m_hbm, m_ref),
        (n_hbm, n_ref),
    )
    head_loads = group(2, (wq_hbm, wq_ref), (wk_hbm, wk_ref), (wv_hbm, wv_ref))
    c_loads = group(3, *((c_hbm.at[t], c_buf.at[t]) for t in range(rows)))
    mix_loads = group(4, (mix_hbm, mix_buf))
    route_loads = group(5, (routes_hbm, routes_ref), (scale_hbm, scale_ref), (fgain_hbm, fgain_ref))
    dense_loads = group(6, (wb_hbm, wb_ref), (dg_hbm, dg), (du_hbm, du), (dd_hbm, dd))
    expert_loads = group(
        7, (eg_hbm.at[0], eg.at[0]), (eu_hbm.at[0], eu.at[0]), (ed_hbm.at[0], ed.at[0])
    )

    def start(*groups):
        for copies in groups:
            for copy in copies:
                copy.start()

    def finish(copies):
        for copy in copies:
            copy.wait()

    start(first_loads)
    barrier, count = greet()
    start(gate_loads, head_loads, c_loads, mix_loads, route_loads)

    with scope("norm"):
        finish(first_loads)
        tokens = padded(tokens_ref[...].astype(F32), pad_rows)
        normed = rms_scaled(tokens, gain_ref[...]).astype(BF16)
    with scope("gates"):
        finish(gate_loads)
        pre_all = dot_nt(normed, wi_ref[...]) + ib_ref[...]
        fg_all = dot_nt(normed, wf_ref[...]) + fb_ref[...]
        fg_all = jnp.minimum(fg_all, 0.0) - jnp.log(1.0 + jnp.exp(-jnp.abs(fg_all)))
    with scope("qkv"):
        finish(head_loads)
        queries = dot(normed, wq_ref[...]).astype(BF16)
        keys = dot(normed, wk_ref[...]).astype(BF16).astype(F32)
        values = dot(normed, wv_ref[...]).astype(BF16).astype(F32)
    key_scale = dk**-0.5
    row_ids = lax.broadcasted_iota(jnp.int32, (pad_rows, dk), 0)
    per_head = []
    with scope("heads"):
        for h in range(heads):
            pre = column(pre_all, first + h)
            shifted = column(fg_all, first + h) + to_column(m_ref[h : h + 1, :], pad_rows)
            new_m = jnp.maximum(shifted, pre)
            forget = jnp.exp(shifted - new_m)
            inflow = jnp.exp(pre - new_m)
            newm_ref[h : h + 1, :] = to_row(new_m, rows)
            q = queries[:, h * dk : (h + 1) * dk].astype(F32)
            k = keys[:, h * dk : (h + 1) * dk] * (inflow * key_scale)
            v = values[:, h * dv : (h + 1) * dv]
            new_n = forget * padded(n_ref[:, h, :], pad_rows) + k
            newn_ref[:, h, :] = new_n[:rows]
            denom = jnp.maximum(jnp.abs(jnp.sum(q * new_n, axis=1, keepdims=True)), 1.0)
            inner = jnp.sum(q * k, axis=1, keepdims=True)
            wide_q = jnp.concatenate([jnp.where(row_ids == t, q, 0.0) for t in range(rows)], axis=1)
            per_head.append((forget, k, v, denom, inner, wide_q.astype(BF16)))
    with scope("readout"):
        pltpu.make_async_copy(c_hbm, c_buf, load_sem.at[3]).wait()
        outs = []
        for h in range(heads):
            forget, _, v, denom, inner, wide_q = per_head[h]
            memory = c_buf[:, h].reshape(rows * dk, dv).astype(BF16)
            outs.append((forget * dot(wide_q, memory) + inner * v) / denom)
        head_out = jnp.concatenate(outs, axis=1).astype(BF16)
    with scope("mix"):
        finish(mix_loads)
        part = dot(head_out, mix_buf[...]).astype(BF16).astype(F32)
        part_send[...] = pack(part, rows).astype(BF16)
    start(dense_loads, expert_loads)
    with scope("barrier"):
        pl.semaphore_wait(barrier, count)

    def mix_copy(dy):
        return remote(part_send, mixed.at[dy - 1], mix_s.at[dy - 1], mix_r.at[dy - 1], at(0, 0, dy, 1))

    for dy in other_planes:
        send(mix_copy(dy))

    def expert_copies(dc):
        return [
            remote(src.at[0], dst.at[dc], e_s.at[dc - 1, i], e_r.at[dc - 1, i], core_at(dc))
            for i, (src, dst) in enumerate(((eg_hbm, eg), (eu_hbm, eu), (ed_hbm, ed)))
        ]

    for dc in range(1, nc):
        for copy in expert_copies(dc):
            send(copy)

    with scope("routes"):
        finish(route_loads)
        scale = scale_ref[...].astype(F32)
        route_weight = scale / jnp.sum(scale, axis=0, keepdims=True)
        experts = own_w.shape[0] * nc
        ids = lax.broadcasted_iota(jnp.int32, (experts, rows), 0)
        table = jnp.zeros((experts, rows), F32)
        for k in range(routes_ref.shape[0]):
            table = table + jnp.where(ids == routes_ref[k : k + 1, :], route_weight[k : k + 1, :], 0.0)
        table = jnp.concatenate([table, jnp.zeros((experts, own_w.shape[2] - rows), F32)], axis=1)
        for e in range(experts):
            own_w[e // nc, e % nc : e % nc + 1, :] = table[e : e + 1, :]

        def w_copy(dz, dx):
            return remote(
                own_w.at[place(dz, dx, 1)],
                weights.at[slot(dz, dx)],
                w_s.at[0],
                w_r.at[0],
                at(dz, dx, 0, 1),
            )

        for dz, dx in other_places:
            w_copy(dz, dx).start()

    with scope("ywait"):
        total = part
        for dy in other_planes:
            mix_copy(dy).wait_recv()
            total = total + unpack(mixed[dy - 1].astype(F32), rows)
    with scope("norm2"):
        residual = tokens + total.astype(BF16).astype(F32)
        ffn_f32 = rms_scaled(residual, fgain_ref[...])
        ffn_in = ffn_f32.astype(BF16)
        block_send[...] = pack(ffn_in.astype(F32), rows).astype(BF16)
        inputs_ref[:pad_rows] = ffn_in

    def g_copy(dz, dx, there):
        return remote(block_send, blocks.at[slot(dz, dx)], g_s.at[0], g_r.at[0], at_place(there, 0, 1))

    for step in far_first(1):
        g_copy(*step).start()

    with scope("dense"):
        finish(dense_loads)
        dense_hidden = (jax.nn.silu(dot(ffn_in, dg[...])) * dot(ffn_in, du[...])).astype(BF16)
        wb = wb_ref[...].astype(F32)
        lanes = wb.shape[1]
        wide = ffn_in.astype(F32)
        branch = jnp.zeros((pad_rows, lanes), F32)
        for i in range(wb.shape[0]):
            branch = branch + wide[:, i * lanes : (i + 1) * lanes] * wb[i : i + 1, :]
        branch = jax.nn.sigmoid(jnp.sum(branch, axis=1, keepdims=True))

        def dense_part(dy):
            cols = pl.ds(pl.multiple_of(plane(dy, -1) * cw, cw), cw)
            return dot(dense_hidden, dd[:, cols]) * branch

        dense = [dense_part(dy) for dy in range(ntp)]
        own = dense[0]
        for j in range(ntp):
            own = own + jnp.where(tp == j, residual[:, j * cw : (j + 1) * cw], 0.0)

    with scope("newc"):
        for h in range(heads):
            forget, k, v, _, _, _ = per_head[h]
            k_t = k.T
            for t in range(rows):
                newc_ref[t, h] = forget[t : t + 1] * c_buf[t, h] + k_t[:, t : t + 1] * v[t : t + 1]

    with scope("factor"):
        all_weights = whole(weights, weights, w_s.at[0], w_r.at[0])
        all_blocks = whole(blocks, blocks, g_s.at[0], g_r.at[0])
        all_results = whole(ret_send, ret, r_s.at[0], r_r.at[0])
        all_weights.wait_recv()
        factors = []
        for dc in range(nc):
            core = lax.rem(c + dc, nc)
            factors.append(
                jnp.concatenate(
                    [
                        to_column(
                            own_w[place(0, 0, 1), pl.ds(core, 1), :]
                            if (dz, dx) == (0, 0)
                            else weights[slot(dz, dx), pl.ds(core, 1), :],
                            pad_rows,
                        )
                        for dz in range(nz)
                        for dx in range(nx)
                    ],
                    axis=0,
                )
            )
    with scope("gwait"):
        all_blocks.wait_recv()
        for dz, dx in other_places:
            at_row = (dz * nx + dx) * pad_rows
            block = blocks[slot(dz, dx)].astype(F32)
            inputs_ref[at_row : at_row + pad_rows] = unpack(block, rows).astype(BF16)
    hidden = []
    for dc in range(nc):
        with scope("wwait"):
            if dc == 0:
                finish(expert_loads)
            else:
                for copy in expert_copies(dc):
                    copy.wait_recv()
        with scope("expert"):
            inputs = inputs_ref[...]
            gate = jnp.minimum(dot(inputs, eg[dc]), CLAMP_LIMIT)
            up = jnp.clip(dot(inputs, eu[dc]), -CLAMP_LIMIT, CLAMP_LIMIT)
            act = gate * jax.nn.sigmoid(SWISH_ALPHA * gate) * (up + 1.0)
            hidden.append((act * factors[dc]).astype(BF16))

    def r_copy(dz, dx, there, dy):
        at_slot = slot(dz, dx, dy)
        return remote(
            ret_send.at[at_slot], ret.at[at_slot], r_s.at[0], r_r.at[0], at_place(there, dy, -1)
        )

    order = far_first(-1)
    late = order[-nx:] if nz > 1 else []
    early = order[: len(order) - len(late)]
    for dy in other_planes[::-1] + [0]:
        with scope("down"):
            cols = pl.ds(pl.multiple_of(plane(dy, -1) * cw, cw), cw)
            result = dot(hidden[0], ed[0, :, cols])
            for dc in range(1, nc):
                result = result + dot(hidden[dc], ed[dc, :, cols])
            for dz, dx in places:
                at_row = (dz * nx + dx) * pad_rows
                value = result[at_row : at_row + pad_rows]
                if (dz, dx, dy) == (0, 0, 0):
                    own = own + value
                    continue
                if (dz, dx) == (0, 0):
                    value = value + dense[dy]
                ret_send[slot(dz, dx, dy)] = pack(value, rows).astype(BF16)
            for dz, dx, there in early:
                r_copy(dz, dx, there, dy).start()
            if dy > 0:
                r_copy(0, 0, place(0, 0, -1), dy).start()
    for dy in other_planes[::-1] + [0]:
        for dz, dx, there in late:
            r_copy(dz, dx, there, dy).start()

    with scope("final"):
        all_results.wait_recv()
        total = ret[0].astype(F32)
        for i in range(1, ret.shape[0]):
            total = total + ret[i].astype(F32)
        own = own + unpack(total, rows)
        out_ref[...] = own[:rows].astype(BF16)
    with scope("sendwait"):
        for copy in pending:
            copy.wait_send()
        for copy in (all_weights, all_blocks, all_results):
            copy.wait_send()


def store_kernel(out_v, c_v, n_v, m_v, out_h, c_h, n_h, m_h, sem):
    copies = [
        pltpu.make_async_copy(src, dst, sem.at[0])
        for src, dst in ((out_v, out_h), (n_v, n_h), (m_v, m_h))
    ]
    states = [pltpu.make_async_copy(c_v.at[t], c_h.at[t], sem.at[1]) for t in range(c_v.shape[0])]
    for copy in copies + states:
        copy.start()
    for copy in copies:
        copy.wait()
    pltpu.make_async_copy(c_v, c_h, sem.at[1]).wait()


def local(
    sizes,
    tokens,
    norm_gain,
    w_query,
    w_key,
    w_value,
    w_input_gate,
    w_forget_gate,
    input_bias,
    forget_bias,
    state_c,
    state_n,
    state_m,
    w_mixer_out,
    ffn_gain,
    routes,
    route_scale,
    w_expert_gate,
    w_expert_up,
    w_expert_down,
    w_dense_gate,
    w_dense_up,
    w_dense_down,
    w_branch_gate,
):
    nz, nx, nc, ntp = sizes
    rows, width = tokens.shape
    pad_rows = -(-rows // 16) * 16
    cw = width // ntp
    vmem = pl.BlockSpec(memory_space=pltpu.VMEM)
    hbm = pl.BlockSpec(memory_space=pl.ANY)
    dma = pltpu.SemaphoreType.DMA
    wide_block = block_shape(rows, pad_rows, width)
    slim_block = block_shape(rows, pad_rows, cw)
    planes = max(1, ntp - 1)
    outs = pl.pallas_call(
        functools.partial(layer_kernel, sizes),
        name="layer",
        out_shape=(
            pltpu.VMEM((rows, cw), BF16),
            pltpu.VMEM(state_c.shape, F32),
            pltpu.VMEM(state_n.shape, F32),
            pltpu.VMEM(state_m.shape[::-1], F32),
        ),
        in_specs=[hbm] * 23,
        out_specs=(vmem,) * 4,
        scratch_shapes=[
            pltpu.VMEM(tokens.shape, BF16),
            pltpu.VMEM((1, width), F32),
            pltpu.VMEM(w_input_gate.shape[::-1], BF16),
            pltpu.VMEM(w_forget_gate.shape[::-1], BF16),
            pltpu.VMEM((1, input_bias.shape[0]), F32),
            pltpu.VMEM((1, forget_bias.shape[0]), F32),
            pltpu.VMEM(state_m.shape[::-1], F32),
            pltpu.VMEM(state_n.shape, F32),
            pltpu.VMEM(w_query.shape, BF16),
            pltpu.VMEM(w_key.shape, BF16),
            pltpu.VMEM(w_value.shape, BF16),
            pltpu.VMEM(state_c.shape, F32),
            pltpu.VMEM(w_mixer_out.shape, BF16),
            pltpu.VMEM((1, width), F32),
            pltpu.VMEM(routes.shape[::-1], jnp.int32),
            pltpu.VMEM(route_scale.shape[::-1], BF16),
            pltpu.VMEM((width // 128, 128), BF16),
            pltpu.VMEM(w_dense_gate.shape, BF16),
            pltpu.VMEM(w_dense_up.shape, BF16),
            pltpu.VMEM(w_dense_down.shape, BF16),
            pltpu.VMEM((nc,) + w_expert_gate.shape[1:], BF16),
            pltpu.VMEM((nc,) + w_expert_up.shape[1:], BF16),
            pltpu.VMEM((nc,) + w_expert_down.shape[1:], BF16),
            pltpu.VMEM(wide_block, BF16),
            pltpu.VMEM((planes,) + wide_block, BF16),
            pltpu.VMEM((nz * nx, nc, 128), F32),
            pltpu.VMEM((nz * nx - 1, nc, 128), F32),
            pltpu.VMEM(wide_block, BF16),
            pltpu.VMEM((nz * nx - 1,) + wide_block, BF16),
            pltpu.VMEM((nz * nx * pad_rows, width), BF16),
            pltpu.VMEM((ntp * nz * nx - 1,) + slim_block, BF16),
            pltpu.VMEM((ntp * nz * nx - 1,) + slim_block, BF16),
            dma((8,)),
            dma((planes,)),
            dma((planes,)),
            dma((1,)),
            dma((1,)),
            dma((1,)),
            dma((1,)),
            dma((max(1, nc - 1), 3)),
            dma((max(1, nc - 1), 3)),
            dma((1,)),
            dma((1,)),
        ],
        compiler_params=pltpu.CompilerParams(
            vmem_limit_bytes=VMEM_LIMIT, collective_id=0, has_side_effects=True
        ),
    )(
        tokens,
        norm_gain.reshape(1, width),
        w_input_gate.T,
        w_forget_gate.T,
        input_bias.reshape(1, -1),
        forget_bias.reshape(1, -1),
        state_m.T,
        state_n,
        w_query,
        w_key,
        w_value,
        state_c,
        w_mixer_out,
        ffn_gain.reshape(1, width),
        routes.T,
        route_scale.T,
        w_branch_gate.reshape(width // 128, 128),
        w_dense_gate,
        w_dense_up,
        w_dense_down,
        w_expert_gate,
        w_expert_up,
        w_expert_down,
    )
    output, new_c, new_n, new_m = pl.pallas_call(
        store_kernel,
        name="store",
        out_shape=(
            jax.ShapeDtypeStruct((rows, cw), BF16),
            jax.ShapeDtypeStruct(state_c.shape, F32),
            jax.ShapeDtypeStruct(state_n.shape, F32),
            jax.ShapeDtypeStruct(state_m.shape[::-1], F32),
        ),
        in_specs=[vmem] * 4,
        out_specs=(hbm,) * 4,
        scratch_shapes=[dma((2,))],
        compiler_params=pltpu.CompilerParams(vmem_limit_bytes=1024 * 1024),
    )(*outs)
    return (output, new_c, new_n, new_m.T)


def solution(mesh):
    n_ep, n_tp = mesh.shape["ep"], mesh.shape["tp"]
    n_core = 2 if n_ep % 2 == 0 else 1
    n_x = n_tp if n_ep % (n_core * n_tp) == 0 else 1
    sizes = (n_ep // (n_core * n_x), n_x, n_core, n_tp)
    in_specs = (
        P("ep", None),
        P(),
        P(None, "tp"),
        P(None, "tp"),
        P(None, "tp"),
        P(),
        P(),
        P(),
        P(),
        P("ep", "tp", None, None),
        P("ep", "tp", None),
        P("ep", "tp"),
        P("tp", None),
        P(),
        P("ep", None),
        P("ep", None),
        P("ep", None, "tp"),
        P("ep", None, "tp"),
        P("ep", "tp", None),
        P(None, "tp"),
        P(None, "tp"),
        P("tp", None),
        P(),
    )
    out_specs = (P("ep", "tp"), P("ep", "tp", None, None), P("ep", "tp", None), P("ep", "tp"))
    return jax.shard_map(
        functools.partial(local, sizes),
        mesh=mesh,
        in_specs=in_specs,
        out_specs=out_specs,
        check_vma=False,
    )
```

```python
import functools

import jax
import jax.numpy as jnp
from jax import lax
from jax.experimental import pallas as pl
from jax.experimental.pallas import tpu as pltpu
from jax.sharding import PartitionSpec as P

EPSILON = 1e-06
CLAMP_LIMIT = 7.0
SWISH_ALPHA = 1.702
MESH = pl.DeviceIdType.MESH
F32 = jnp.float32
BF16 = jnp.bfloat16
VMEM_LIMIT = 60000 * 1024
PIECES = 4
scope = jax.named_scope


def padded(values, rows):
    extra = rows - values.shape[0]
    if extra == 0:
        return values
    return jnp.concatenate([values, jnp.zeros((extra, values.shape[1]), values.dtype)], axis=0)


def dot(left, right):
    return jnp.dot(left, right, preferred_element_type=F32)


def dot_nt(left, right):
    return lax.dot_general(left, right, (((1,), (1,)), ((), ())), preferred_element_type=F32)


def rms_scaled(values, gain):
    scale = lax.rsqrt(jnp.mean(values * values, axis=-1, keepdims=True) + EPSILON)
    return values * scale * gain


def to_column(row, rows):
    shape = (rows, row.shape[1])
    same = lax.broadcasted_iota(jnp.int32, shape, 0) == lax.broadcasted_iota(jnp.int32, shape, 1)
    return jnp.sum(jnp.where(same, row, 0.0), axis=1, keepdims=True)


def to_row(col, lanes):
    shape = (col.shape[0], lanes)
    same = lax.broadcasted_iota(jnp.int32, shape, 0) == lax.broadcasted_iota(jnp.int32, shape, 1)
    return jnp.sum(jnp.where(same, col, 0.0), axis=0, keepdims=True)


def column(values, index):
    lanes = lax.broadcasted_iota(jnp.int32, values.shape, 1)
    return jnp.sum(jnp.where(lanes == index, values, 0.0), axis=1, keepdims=True)


def dense_rows(rows):
    return 8 < rows <= 12


def block_shape(rows, pad_rows, width):
    return (8, width + width // 2) if dense_rows(rows) else (pad_rows, width)


def pack(values, rows):
    if not dense_rows(rows):
        return values
    half = values.shape[1] // 2
    low, high = values[8:16, :half], values[8:16, half:]
    top = lax.broadcasted_iota(jnp.int32, low.shape, 0) < 4
    return jnp.concatenate([values[:8], jnp.where(top, low, pltpu.roll(high, 4, 0))], axis=1)


def unpack(block, rows):
    if not dense_rows(rows):
        return block
    width = block.shape[1] // 3 * 2
    tail = block[:, width:]
    return jnp.concatenate(
        [block[:, :width], jnp.concatenate([tail, pltpu.roll(tail, 4, 0)], axis=1)], axis=0
    )


def partner(index, step, size, sign):
    if size & (size - 1):
        return lax.rem(index + sign * step + size, size)
    bit = 1
    while bit < size:
        if step & bit:
            index = index + bit * (1 - 2 * lax.rem(lax.div(index, bit), 2))
        bit *= 2
    return index


def step_between(a, b, size):
    if size & (size - 1):
        return lax.rem(b - a + size, size)
    step, bit = 0, 1
    while bit < size:
        step = step + bit * lax.rem(lax.div(a, bit) + lax.div(b, bit), 2)
        bit *= 2
    return step


def layer_kernel(
    sizes,
    tokens_hbm,
    gain_hbm,
    wi_hbm,
    wf_hbm,
    ib_hbm,
    fb_hbm,
    m_hbm,
    n_hbm,
    wq_hbm,
    wk_hbm,
    wv_hbm,
    c_hbm,
    mix_hbm,
    fgain_hbm,
    routes_hbm,
    scale_hbm,
    wb_hbm,
    dg_hbm,
    du_hbm,
    dd_hbm,
    eg_hbm,
    eu_hbm,
    ed_hbm,
    out_ref,
    newc_ref,
    newn_ref,
    newm_ref,
    tokens_ref,
    gain_ref,
    wi_ref,
    wf_ref,
    ib_ref,
    fb_ref,
    m_ref,
    n_ref,
    wq_ref,
    wk_ref,
    wv_ref,
    c_buf,
    mix_buf,
    fgain_ref,
    routes_ref,
    scale_ref,
    wb_ref,
    dg,
    du,
    dd,
    eg,
    eu,
    ed,
    part_send,
    mixed,
    own_w,
    weights,
    block_send,
    blocks,
    inputs_ref,
    dense_send,
    dense_ref,
    ret_send,
    ret,
    load_sem,
    mix_s,
    mix_r,
    w_s,
    w_r,
    g_s,
    g_r,
    e_s,
    e_r,
    d_s,
    d_r,
    r_s,
    r_r,
):
    nz, nx, nc, ntp = sizes
    ep = lax.axis_index("ep")
    tp = lax.axis_index("tp")
    c = lax.rem(ep, nc)
    x = lax.rem(lax.div(ep, nc), nx)
    z = lax.div(ep, nc * nx)
    rows, width = tokens_ref.shape
    pad_rows = inputs_ref.shape[1] // (nz * nx)
    heads = m_ref.shape[0]
    dk, dv = c_buf.shape[2], c_buf.shape[3]
    cw = width // ntp
    first = tp * heads
    main = nc - 1
    is_main = lax.div(c + 1, nc)
    layer = main - c
    count_places = nz * nx

    def on_main(body):
        return body() if nc == 1 else pl.when(c == main)(body)

    def on_side(body):
        return None if nc == 1 else pl.when(c != main)(body)

    def place(dz, dx, sign):
        return partner(z, dz, nz, sign) * nx + partner(x, dx, nx, sign)

    def plane(dy, sign):
        return partner(tp, dy, ntp, sign)

    def device(there, core, dy, sign):
        return {"ep": there * nc + core, "tp": plane(dy, sign)}

    def remote(src, dst, send, recv, device):
        return pltpu.make_async_remote_copy(
            src_ref=src, dst_ref=dst, send_sem=send, recv_sem=recv, device_id=device, device_id_type=MESH
        )

    def slot(dz, dx, dy=0):
        return (dy * nz + dz) * nx + dx

    here = place(0, 0, 1)
    pending = []

    def send(copy):
        copy.start()
        pending.append(copy)

    def whole(ref, sem):
        return remote(ref, ref, sem, sem, device(place(nz - 1, nx - 1, 1), c, ntp - 1, 1))

    def far_first(sign):
        upper = lax.div(2 * z, nz)
        steps = [(0, dx, place(0, dx, sign)) for dx in range(1, nx)]
        for i in range(nz - 1):
            down = nz - 1 - i - lax.div(i + z + 1, nz)
            up = i + 1 - lax.div(nz - 1 - i + z, nz)
            there = upper * up + (1 - upper) * down
            dz = step_between(z, there, nz) if sign > 0 else step_between(there, z, nz)
            for dx in range(nx - 1, -1, -1):
                steps.append((dz, dx, there * nx + partner(x, dx, nx, sign)))
        return steps

    places = [(dz, dx) for dz in range(nz - 1, -1, -1) for dx in range(nx - 1, -1, -1)]
    other_places = places[:-1]
    other_planes = list(range(1, ntp))

    def greet():
        barrier = pltpu.get_barrier_semaphore()

        def signal(there):
            pl.semaphore_signal(barrier, inc=1, device_id=there, device_id_type=MESH)

        for dy in other_planes:
            signal(device(here, c, dy, 1))

        @on_main
        def _():
            for dz, dx in places:
                for core in range(nc):
                    if (dz, dx, core) != (0, 0, main):
                        signal(device(place(dz, dx, 1), core, 0, 1))

        return barrier, len(other_planes) + count_places - is_main

    def group(index, *pairs):
        return [pltpu.make_async_copy(src, dst, load_sem.at[index]) for src, dst in pairs]

    first_loads = group(0, (tokens_hbm, tokens_ref), (gain_hbm, gain_ref))
    gate_loads = group(
        1,
        (wi_hbm, wi_ref),
        (wf_hbm, wf_ref),
        (ib_hbm, ib_ref),
        (fb_hbm, fb_ref),
        (m_hbm, m_ref),
        (n_hbm, n_ref),
    )
    q_loads = group(2, (wq_hbm, wq_ref), (wk_hbm, wk_ref))
    v_loads = group(8, (wv_hbm, wv_ref))
    c_loads = group(3, *((c_hbm.at[t], c_buf.at[t]) for t in range(rows)))
    mix_loads = group(4, (mix_hbm, mix_buf))
    route_loads = group(5, (routes_hbm, routes_ref), (scale_hbm, scale_ref), (fgain_hbm, fgain_ref))
    dense_loads = group(6, (wb_hbm, wb_ref), (dg_hbm, dg), (du_hbm, du), (dd_hbm, dd))
    expert_loads = group(
        7, (eg_hbm.at[0], eg.at[main]), (eu_hbm.at[0], eu.at[main]), (ed_hbm.at[0], ed.at[main])
    )

    def start(*groups):
        for copies in groups:
            for copy in copies:
                copy.start()

    def finish(copies):
        for copy in copies:
            copy.wait()

    start(first_loads)
    barrier, count = greet()
    start(gate_loads, q_loads, v_loads, c_loads, mix_loads, route_loads)

    with scope("norm"):
        finish(first_loads)
        tokens = padded(tokens_ref[...].astype(F32), pad_rows)
        normed = rms_scaled(tokens, gain_ref[...]).astype(BF16)
    with scope("gates"):
        finish(gate_loads)
        pre_all = dot_nt(normed, wi_ref[...]) + ib_ref[...]
        fg_all = dot_nt(normed, wf_ref[...]) + fb_ref[...]
        fg_all = jnp.minimum(fg_all, 0.0) - jnp.log(1.0 + jnp.exp(-jnp.abs(fg_all)))
    row_ids = lax.broadcasted_iota(jnp.int32, (pad_rows, dk), 0)
    with scope("queries"):
        finish(q_loads)
        queries = dot(normed, wq_ref[...]).astype(BF16).astype(F32)
        keys = dot(normed, wk_ref[...]).astype(BF16).astype(F32)
        wide = [
            jnp.concatenate(
                [jnp.where(row_ids == t, queries[:, h * dk : (h + 1) * dk], 0.0) for t in range(rows)], axis=1
            ).astype(BF16)
            for h in range(heads)
        ]
    with scope("readout"):
        pltpu.make_async_copy(c_hbm, c_buf, load_sem.at[3]).wait()
        finish(v_loads)
    values = dot(normed, wv_ref[...]).astype(BF16).astype(F32)
    reads = [dot(wide[h], c_buf[:, h].reshape(rows * dk, dv).astype(BF16)) for h in range(heads)]
    key_scale = dk**-0.5
    per_head, outs = [], []
    with scope("heads"):
        for h in range(heads):
            pre = column(pre_all, first + h)
            shifted = column(fg_all, first + h) + to_column(m_ref[h : h + 1, :], pad_rows)
            new_m = jnp.maximum(shifted, pre)
            forget = jnp.exp(shifted - new_m)
            inflow = jnp.exp(pre - new_m)
            newm_ref[h : h + 1, :] = to_row(new_m, rows)
            q = queries[:, h * dk : (h + 1) * dk]
            k = keys[:, h * dk : (h + 1) * dk] * (inflow * key_scale)
            v = values[:, h * dv : (h + 1) * dv]
            new_n = forget * padded(n_ref[:, h, :], pad_rows) + k
            newn_ref[:, h, :] = new_n[:rows]
            denom = jnp.maximum(jnp.abs(jnp.sum(q * new_n, axis=1, keepdims=True)), 1.0)
            inner = jnp.sum(q * k, axis=1, keepdims=True)
            outs.append((forget * reads[h] + inner * v) / denom)
            per_head.append((forget, k, v))
        head_out = jnp.concatenate(outs, axis=1).astype(BF16)
    with scope("mix"):
        finish(mix_loads)
        part = dot(head_out, mix_buf[...]).astype(BF16).astype(F32)
        part_send[...] = pack(part, rows).astype(BF16)
    start(dense_loads)
    on_main(lambda: start(expert_loads))
    with scope("barrier"):
        pl.semaphore_wait(barrier, count)

    def mix_copy(dy):
        return remote(
            part_send, mixed.at[dy - 1], mix_s.at[dy - 1], mix_r.at[dy - 1], device(here, c, dy, 1)
        )

    for dy in other_planes:
        send(mix_copy(dy))

    def expert_copies(core, pieces=1):
        copies = []
        for i, (src, dst) in enumerate(((eg_hbm, eg), (eu_hbm, eu), (ed_hbm, ed))):
            size = src.shape[1] // pieces
            for piece in range(pieces):
                part_rows = pl.ds(piece * size, size)
                copies.append(
                    remote(
                        src.at[0, part_rows],
                        dst.at[core, part_rows],
                        e_s.at[core, i],
                        e_r.at[core, i],
                        device(here, main, 0, 1),
                    )
                )
        return copies

    on_side(lambda: start(expert_copies(c, PIECES)))

    with scope("routes"):
        finish(route_loads)
        scale = scale_ref[...].astype(F32)
        route_weight = scale / jnp.sum(scale, axis=0, keepdims=True)
        experts = own_w.shape[0] * nc
        ids = lax.broadcasted_iota(jnp.int32, (experts, rows), 0)
        table = jnp.zeros((experts, rows), F32)
        for k in range(routes_ref.shape[0]):
            table = table + jnp.where(ids == routes_ref[k : k + 1, :], route_weight[k : k + 1, :], 0.0)
        table = jnp.concatenate([table, jnp.zeros((experts, own_w.shape[2] - rows), F32)], axis=1)
        for e in range(experts):
            own_w[e // nc, e % nc : e % nc + 1, :] = table[e : e + 1, :]

        def w_copy(dz, dx):
            there = place(dz, dx, 1)
            return remote(
                own_w.at[there],
                weights.at[layer, slot(dz, dx)],
                w_s.at[0],
                w_r.at[layer],
                device(there, main, 0, 1),
            )

        for dz, dx in other_places:
            w_copy(dz, dx).start()
        on_side(lambda: w_copy(0, 0).start())

        @on_main
        def _():
            weights[0, 0] = own_w[here]

    with scope("ywait"):
        total = part
        for dy in other_planes:
            mix_copy(dy).wait_recv()
            total = total + unpack(mixed[dy - 1].astype(F32), rows)
    with scope("norm2"):
        residual = tokens + total.astype(BF16).astype(F32)
        ffn_f32 = rms_scaled(residual, fgain_ref[...])
        ffn_in = ffn_f32.astype(BF16)
        block_send[...] = pack(ffn_in.astype(F32), rows).astype(BF16)

        @on_main
        def _():
            inputs_ref[0, :pad_rows] = ffn_in

    def g_copy(dz, dx, there):
        return remote(
            block_send, blocks.at[layer, slot(dz, dx)], g_s.at[0], g_r.at[layer], device(there, main, 0, 1)
        )

    for step in far_first(1):
        g_copy(*step).start()
    on_side(lambda: g_copy(0, 0, here).start())

    def d_copy(dy):
        return remote(
            dense_send.at[dy - 1],
            dense_ref.at[dy - 1],
            d_s.at[dy - 1],
            d_r.at[dy - 1],
            device(here, c, dy, -1),
        )

    with scope("dense"):
        finish(dense_loads)
        dense_hidden = (jax.nn.silu(dot(ffn_in, dg[...])) * dot(ffn_in, du[...])).astype(BF16)
        wb = wb_ref[...].astype(F32)
        lanes = wb.shape[1]
        wide_in = ffn_in.astype(F32)
        branch = jnp.zeros((pad_rows, lanes), F32)
        for i in range(wb.shape[0]):
            branch = branch + wide_in[:, i * lanes : (i + 1) * lanes] * wb[i : i + 1, :]
        branch = jax.nn.sigmoid(jnp.sum(branch, axis=1, keepdims=True))

        def dense_part(dy):
            cols = pl.ds(pl.multiple_of(plane(dy, -1) * cw, cw), cw)
            return dot(dense_hidden, dd[:, cols]) * branch

        dense = [dense_part(dy) for dy in range(ntp)]
        for dy in other_planes:
            dense_send[dy - 1] = pack(dense[dy], rows).astype(BF16)
            send(d_copy(dy))
        own = dense[0]
        for j in range(ntp):
            own = own + jnp.where(tp == j, residual[:, j * cw : (j + 1) * cw], 0.0)

    with scope("newc"):
        for h in range(heads):
            forget, k, v = per_head[h]
            k_t = k.T
            for t in range(rows):
                newc_ref[t, h] = forget[t : t + 1] * c_buf[t, h] + k_t[:, t : t + 1] * v[t : t + 1]

    def r_copy(dz, dx, there, dy, core):
        at_slot = slot(dz, dx, dy)
        return remote(
            ret_send.at[(main - core) * ret.shape[0] + at_slot],
            ret.at[at_slot],
            r_s.at[0],
            r_r.at[0],
            device(there, core, dy, -1),
        )

    def run_experts(core):
        index = main - core
        skip = 1 if core == main else 0
        with scope(f"factor{core}"):
            whole(weights.at[index, skip:], w_r.at[index]).wait_recv()
            factors = [
                jnp.concatenate(
                    [
                        to_column(weights[index, k, expert : expert + 1, :], pad_rows)
                        for k in range(count_places)
                    ],
                    axis=0,
                )
                for expert in range(nc)
            ]
        with scope(f"gwait{core}"):
            whole(blocks.at[index, skip:], g_r.at[index]).wait_recv()
        with scope(f"inputs{core}"):
            for k in range(skip, count_places):
                block = blocks[index, k].astype(F32)
                inputs_ref[index, k * pad_rows : (k + 1) * pad_rows] = unpack(block, rows).astype(BF16)
        hidden = [None] * nc
        for expert in range(nc - 1, -1, -1):
            if core == main:
                with scope("wwait"):
                    if expert == main:
                        finish(expert_loads)
                    else:
                        for copy in expert_copies(expert)[:2]:
                            copy.wait_recv()
            with scope(f"expert{core}"):
                inputs = inputs_ref[index]
                gate = jnp.minimum(dot(inputs, eg[expert]), CLAMP_LIMIT)
                up = jnp.clip(dot(inputs, eu[expert]), -CLAMP_LIMIT, CLAMP_LIMIT)
                act = gate * jax.nn.sigmoid(SWISH_ALPHA * gate) * (up + 1.0)
                hidden[expert] = (act * factors[expert]).astype(BF16)
        if core == main:
            with scope("wwait"):
                for expert in range(main):
                    expert_copies(expert)[2].wait_recv()
        order = far_first(-1)
        early = order[: 2 * nx - 1]
        late = order[2 * nx - 1 :]
        for dy in other_planes[::-1] + [0]:
            with scope(f"down{core}"):
                cols = pl.ds(pl.multiple_of(plane(dy, -1) * cw, cw), cw)
                result = dot(hidden[0], ed[0, :, cols])
                for expert in range(1, nc):
                    result = result + dot(hidden[expert], ed[expert, :, cols])
                for dz, dx in places:
                    at_row = (dz * nx + dx) * pad_rows
                    value = pack(result[at_row : at_row + pad_rows], rows).astype(BF16)
                    if skip and (dz, dx, dy) == (0, 0, 0):
                        ret[0] = value
                    else:
                        ret_send[index * ret.shape[0] + slot(dz, dx, dy)] = value
                for dz, dx, there in early:
                    r_copy(dz, dx, there, dy, core).start()
                if dy > 0 or not skip:
                    r_copy(0, 0, here, dy, core).start()
        for dz, dx, there in late:
            for dy in other_planes[::-1] + [0]:
                r_copy(dz, dx, there, dy, core).start()

    @on_main
    def _():
        for core in range(main, -1, -1):
            run_experts(core)

    with scope("final"):
        for dy in other_planes:
            d_copy(dy).wait_recv()
        on_main(lambda: whole(ret.at[1:], r_r.at[0]).wait_recv())
        on_side(lambda: whole(ret, r_r.at[0]).wait_recv())
        total = ret[0].astype(F32)
        for i in range(1, ret.shape[0]):
            total = total + ret[i].astype(F32)
        for dy in other_planes:
            total = total + dense_ref[dy - 1].astype(F32)
        own = own + unpack(total, rows)
        out_ref[...] = own[:rows].astype(BF16)
    with scope("sendwait"):
        for copy in pending:
            copy.wait_send()

        @on_main
        def _():
            whole(weights.at[0, 1:], w_s.at[0]).wait_send()
            whole(blocks.at[0, 1:], g_s.at[0]).wait_send()
            whole(ret_send.at[1:], r_s.at[0]).wait_send()

        @on_side
        def _():
            whole(weights.at[0], w_s.at[0]).wait_send()
            whole(blocks.at[0], g_s.at[0]).wait_send()
            for copy in expert_copies(c):
                copy.wait_send()


def store_kernel(out_v, c_v, n_v, m_v, out_h, c_h, n_h, m_h, sem):
    copies = [
        pltpu.make_async_copy(src, dst, sem.at[0])
        for src, dst in ((out_v, out_h), (n_v, n_h), (m_v, m_h))
    ]
    states = [pltpu.make_async_copy(c_v.at[t], c_h.at[t], sem.at[1]) for t in range(c_v.shape[0])]
    for copy in copies + states:
        copy.start()
    for copy in copies:
        copy.wait()
    pltpu.make_async_copy(c_v, c_h, sem.at[1]).wait()


def local(
    sizes,
    tokens,
    norm_gain,
    w_query,
    w_key,
    w_value,
    w_input_gate,
    w_forget_gate,
    input_bias,
    forget_bias,
    state_c,
    state_n,
    state_m,
    w_mixer_out,
    ffn_gain,
    routes,
    route_scale,
    w_expert_gate,
    w_expert_up,
    w_expert_down,
    w_dense_gate,
    w_dense_up,
    w_dense_down,
    w_branch_gate,
):
    nz, nx, nc, ntp = sizes
    rows, width = tokens.shape
    pad_rows = -(-rows // 16) * 16
    cw = width // ntp
    vmem = pl.BlockSpec(memory_space=pltpu.VMEM)
    hbm = pl.BlockSpec(memory_space=pl.ANY)
    dma = pltpu.SemaphoreType.DMA
    wide_block = block_shape(rows, pad_rows, width)
    slim_block = block_shape(rows, pad_rows, cw)
    planes = max(1, ntp - 1)
    outs = pl.pallas_call(
        functools.partial(layer_kernel, sizes),
        name="layer",
        out_shape=(
            pltpu.VMEM((rows, cw), BF16),
            pltpu.VMEM(state_c.shape, F32),
            pltpu.VMEM(state_n.shape, F32),
            pltpu.VMEM(state_m.shape[::-1], F32),
        ),
        in_specs=[hbm] * 23,
        out_specs=(vmem,) * 4,
        scratch_shapes=[
            pltpu.VMEM(tokens.shape, BF16),
            pltpu.VMEM((1, width), F32),
            pltpu.VMEM(w_input_gate.shape[::-1], BF16),
            pltpu.VMEM(w_forget_gate.shape[::-1], BF16),
            pltpu.VMEM((1, input_bias.shape[0]), F32),
            pltpu.VMEM((1, forget_bias.shape[0]), F32),
            pltpu.VMEM(state_m.shape[::-1], F32),
            pltpu.VMEM(state_n.shape, F32),
            pltpu.VMEM(w_query.shape, BF16),
            pltpu.VMEM(w_key.shape, BF16),
            pltpu.VMEM(w_value.shape, BF16),
            pltpu.VMEM(state_c.shape, F32),
            pltpu.VMEM(w_mixer_out.shape, BF16),
            pltpu.VMEM((1, width), F32),
            pltpu.VMEM(routes.shape[::-1], jnp.int32),
            pltpu.VMEM(route_scale.shape[::-1], BF16),
            pltpu.VMEM((width // 128, 128), BF16),
            pltpu.VMEM(w_dense_gate.shape, BF16),
            pltpu.VMEM(w_dense_up.shape, BF16),
            pltpu.VMEM(w_dense_down.shape, BF16),
            pltpu.VMEM((nc,) + w_expert_gate.shape[1:], BF16),
            pltpu.VMEM((nc,) + w_expert_up.shape[1:], BF16),
            pltpu.VMEM((nc,) + w_expert_down.shape[1:], BF16),
            pltpu.VMEM(wide_block, BF16),
            pltpu.VMEM((planes,) + wide_block, BF16),
            pltpu.VMEM((nz * nx, nc, 128), F32),
            pltpu.VMEM((nc, nz * nx, nc, 128), F32),
            pltpu.VMEM(wide_block, BF16),
            pltpu.VMEM((nc, nz * nx) + wide_block, BF16),
            pltpu.VMEM((nc, nz * nx * pad_rows, width), BF16),
            pltpu.VMEM((planes,) + slim_block, BF16),
            pltpu.VMEM((planes,) + slim_block, BF16),
            pltpu.VMEM((nc * ntp * nz * nx,) + slim_block, BF16),
            pltpu.VMEM((ntp * nz * nx,) + slim_block, BF16),
            dma((9,)),
            dma((planes,)),
            dma((planes,)),
            dma((1,)),
            dma((nc,)),
            dma((1,)),
            dma((nc,)),
            dma((max(1, nc - 1), 3)),
            dma((max(1, nc - 1), 3)),
            dma((planes,)),
            dma((planes,)),
            dma((1,)),
            dma((1,)),
        ],
        compiler_params=pltpu.CompilerParams(
            vmem_limit_bytes=VMEM_LIMIT, collective_id=0, has_side_effects=True
        ),
    )(
        tokens,
        norm_gain.reshape(1, width),
        w_input_gate.T,
        w_forget_gate.T,
        input_bias.reshape(1, -1),
        forget_bias.reshape(1, -1),
        state_m.T,
        state_n,
        w_query,
        w_key,
        w_value,
        state_c,
        w_mixer_out,
        ffn_gain.reshape(1, width),
        routes.T,
        route_scale.T,
        w_branch_gate.reshape(width // 128, 128),
        w_dense_gate,
        w_dense_up,
        w_dense_down,
        w_expert_gate,
        w_expert_up,
        w_expert_down,
    )
    output, new_c, new_n, new_m = pl.pallas_call(
        store_kernel,
        name="store",
        out_shape=(
            jax.ShapeDtypeStruct((rows, cw), BF16),
            jax.ShapeDtypeStruct(state_c.shape, F32),
            jax.ShapeDtypeStruct(state_n.shape, F32),
            jax.ShapeDtypeStruct(state_m.shape[::-1], F32),
        ),
        in_specs=[vmem] * 4,
        out_specs=(hbm,) * 4,
        scratch_shapes=[dma((2,))],
        compiler_params=pltpu.CompilerParams(vmem_limit_bytes=1024 * 1024),
    )(*outs)
    return (output, new_c, new_n, new_m.T)


def solution(mesh):
    n_ep, n_tp = mesh.shape["ep"], mesh.shape["tp"]
    n_core = 2 if n_ep % 2 == 0 else 1
    n_x = n_tp if n_ep % (n_core * n_tp) == 0 else 1
    sizes = (n_ep // (n_core * n_x), n_x, n_core, n_tp)
    in_specs = (
        P("ep", None),
        P(),
        P(None, "tp"),
        P(None, "tp"),
        P(None, "tp"),
        P(),
        P(),
        P(),
        P(),
        P("ep", "tp", None, None),
        P("ep", "tp", None),
        P("ep", "tp"),
        P("tp", None),
        P(),
        P("ep", None),
        P("ep", None),
        P("ep", None, "tp"),
        P("ep", None, "tp"),
        P("ep", "tp", None),
        P(None, "tp"),
        P(None, "tp"),
        P("tp", None),
        P(),
    )
    out_specs = (P("ep", "tp"), P("ep", "tp", None, None), P("ep", "tp", None), P("ep", "tp"))
    return jax.shard_map(
        functools.partial(local, sizes),
        mesh=mesh,
        in_specs=in_specs,
        out_specs=out_specs,
        check_vma=False,
    )
```

```python
import functools

import jax
import jax.numpy as jnp
from jax import lax
from jax.experimental import pallas as pl
from jax.experimental.pallas import tpu as pltpu
from jax.sharding import PartitionSpec as P

EPSILON = 1e-06
CLAMP_LIMIT = 7.0
SWISH_ALPHA = 1.702
MESH = pl.DeviceIdType.MESH
F32 = jnp.float32
BF16 = jnp.bfloat16
VMEM_LIMIT = 60000 * 1024
PIECES = 4
scope = jax.named_scope


def padded(values, rows):
    extra = rows - values.shape[0]
    if extra == 0:
        return values
    return jnp.concatenate([values, jnp.zeros((extra, values.shape[1]), values.dtype)], axis=0)


def dot(left, right):
    return jnp.dot(left, right, preferred_element_type=F32)


def dot_nt(left, right):
    return lax.dot_general(left, right, (((1,), (1,)), ((), ())), preferred_element_type=F32)


def rms_scaled(values, gain):
    scale = lax.rsqrt(jnp.mean(values * values, axis=-1, keepdims=True) + EPSILON)
    return values * scale * gain


def to_column(row, rows):
    shape = (rows, row.shape[1])
    same = lax.broadcasted_iota(jnp.int32, shape, 0) == lax.broadcasted_iota(jnp.int32, shape, 1)
    return jnp.sum(jnp.where(same, row, 0.0), axis=1, keepdims=True)


def to_row(col, lanes):
    shape = (col.shape[0], lanes)
    same = lax.broadcasted_iota(jnp.int32, shape, 0) == lax.broadcasted_iota(jnp.int32, shape, 1)
    return jnp.sum(jnp.where(same, col, 0.0), axis=0, keepdims=True)


def column(values, index):
    lanes = lax.broadcasted_iota(jnp.int32, values.shape, 1)
    return jnp.sum(jnp.where(lanes == index, values, 0.0), axis=1, keepdims=True)


def dense_rows(rows):
    return 8 < rows <= 12


def block_shape(rows, pad_rows, width):
    return (8, width + width // 2) if dense_rows(rows) else (pad_rows, width)


def pack(values, rows):
    if not dense_rows(rows):
        return values
    half = values.shape[1] // 2
    low, high = values[8:16, :half], values[8:16, half:]
    top = lax.broadcasted_iota(jnp.int32, low.shape, 0) < 4
    return jnp.concatenate([values[:8], jnp.where(top, low, pltpu.roll(high, 4, 0))], axis=1)


def unpack(block, rows):
    if not dense_rows(rows):
        return block
    width = block.shape[1] // 3 * 2
    tail = block[:, width:]
    return jnp.concatenate(
        [block[:, :width], jnp.concatenate([tail, pltpu.roll(tail, 4, 0)], axis=1)], axis=0
    )


def partner(index, step, size, sign):
    if size & (size - 1):
        return lax.rem(index + sign * step + size, size)
    bit = 1
    while bit < size:
        if step & bit:
            index = index + bit * (1 - 2 * lax.rem(lax.div(index, bit), 2))
        bit *= 2
    return index


def step_between(a, b, size):
    if size & (size - 1):
        return lax.rem(b - a + size, size)
    step, bit = 0, 1
    while bit < size:
        step = step + bit * lax.rem(lax.div(a, bit) + lax.div(b, bit), 2)
        bit *= 2
    return step


def layer_kernel(
    sizes,
    tokens_hbm,
    gain_hbm,
    wi_hbm,
    wf_hbm,
    ib_hbm,
    fb_hbm,
    m_hbm,
    n_hbm,
    wq_hbm,
    wk_hbm,
    wv_hbm,
    c_hbm,
    mix_hbm,
    fgain_hbm,
    routes_hbm,
    scale_hbm,
    wb_hbm,
    dg_hbm,
    du_hbm,
    dd_hbm,
    eg_hbm,
    eu_hbm,
    ed_hbm,
    out_ref,
    newc_ref,
    newn_ref,
    newm_ref,
    tokens_ref,
    gain_ref,
    wi_ref,
    wf_ref,
    ib_ref,
    fb_ref,
    m_ref,
    n_ref,
    wq_ref,
    wk_ref,
    wv_ref,
    c_buf,
    mix_buf,
    fgain_ref,
    routes_ref,
    scale_ref,
    wb_ref,
    dg,
    du,
    dd,
    eg,
    eu,
    ed,
    part_send,
    mixed,
    own_w,
    weights,
    block_send,
    blocks,
    inputs_ref,
    dense_send,
    dense_ref,
    ret_send,
    ret,
    load_sem,
    mix_s,
    mix_r,
    w_s,
    w_r,
    g_s,
    g_r,
    e_s,
    e_r,
    d_s,
    d_r,
    r_s,
    r_r,
):
    nz, nx, nc, ntp = sizes
    ep = lax.axis_index("ep")
    tp = lax.axis_index("tp")
    c = lax.rem(ep, nc)
    x = lax.rem(lax.div(ep, nc), nx)
    z = lax.div(ep, nc * nx)
    rows, width = tokens_ref.shape
    pad_rows = inputs_ref.shape[1] // (nz * nx)
    heads = m_ref.shape[0]
    dk, dv = c_buf.shape[2], c_buf.shape[3]
    cw = width // ntp
    first = tp * heads
    main = nc - 1
    is_main = lax.div(c + 1, nc)
    layer = main - c
    count_places = nz * nx

    def on_main(body):
        return body() if nc == 1 else pl.when(c == main)(body)

    def on_side(body):
        return None if nc == 1 else pl.when(c != main)(body)

    def place(dz, dx, sign):
        return partner(z, dz, nz, sign) * nx + partner(x, dx, nx, sign)

    def plane(dy, sign):
        return partner(tp, dy, ntp, sign)

    def device(there, core, dy, sign):
        return {"ep": there * nc + core, "tp": plane(dy, sign)}

    def remote(src, dst, send, recv, device):
        return pltpu.make_async_remote_copy(
            src_ref=src, dst_ref=dst, send_sem=send, recv_sem=recv, device_id=device, device_id_type=MESH
        )

    def slot(dz, dx, dy=0):
        return (dy * nz + dz) * nx + dx

    here = place(0, 0, 1)
    pending = []

    def send(copy):
        copy.start()
        pending.append(copy)

    def whole(ref, sem):
        return remote(ref, ref, sem, sem, device(place(nz - 1, nx - 1, 1), c, ntp - 1, 1))

    def far_first(sign):
        steps = [(dz, dx) for dz in range(nz) for dx in range(nx)][1:]
        steps.sort(key=lambda step: -min(step[0], nz - step[0]) * nx - step[1])
        return [(dz, dx, place(dz, dx, sign)) for dz, dx in steps]

    places = [(dz, dx) for dz in range(nz - 1, -1, -1) for dx in range(nx - 1, -1, -1)]
    other_places = places[:-1]
    other_planes = list(range(1, ntp))

    def greet():
        barrier = pltpu.get_barrier_semaphore()

        def signal(there):
            pl.semaphore_signal(barrier, inc=1, device_id=there, device_id_type=MESH)

        for dy in other_planes:
            signal(device(here, c, dy, 1))

        @on_main
        def _():
            for dz, dx in places:
                for core in range(nc):
                    if (dz, dx, core) != (0, 0, main):
                        signal(device(place(dz, dx, 1), core, 0, 1))

        return barrier, len(other_planes) + count_places - is_main

    def group(index, *pairs):
        return [pltpu.make_async_copy(src, dst, load_sem.at[index]) for src, dst in pairs]

    first_loads = group(0, (tokens_hbm, tokens_ref), (gain_hbm, gain_ref))
    gate_loads = group(
        1,
        (wi_hbm, wi_ref),
        (wf_hbm, wf_ref),
        (ib_hbm, ib_ref),
        (fb_hbm, fb_ref),
        (m_hbm, m_ref),
        (n_hbm, n_ref),
    )
    q_loads = group(2, (wq_hbm, wq_ref), (wk_hbm, wk_ref))
    v_loads = group(7, (wv_hbm, wv_ref))
    c_loads = group(3, *((c_hbm.at[t], c_buf.at[t]) for t in range(rows)))
    mix_loads = group(
        4, (mix_hbm, mix_buf), (routes_hbm, routes_ref), (scale_hbm, scale_ref), (fgain_hbm, fgain_ref)
    )
    dense_loads = group(5, (wb_hbm, wb_ref), (dg_hbm, dg), (du_hbm, du), (dd_hbm, dd))
    expert_loads = group(
        6, (eg_hbm.at[0], eg.at[main]), (eu_hbm.at[0], eu.at[main]), (ed_hbm.at[0], ed.at[main])
    )

    def start(*groups):
        for copies in groups:
            for copy in copies:
                copy.start()

    def finish(copies):
        for copy in copies:
            copy.wait()

    start(first_loads)
    barrier, count = greet()
    start(gate_loads, q_loads, v_loads, c_loads, mix_loads)

    with scope("norm"):
        finish(first_loads)
        tokens = padded(tokens_ref[...].astype(F32), pad_rows)
        normed = rms_scaled(tokens, gain_ref[...]).astype(BF16)
    gate_rows = []
    with scope("gates"):
        finish(gate_loads)
        pre_all = dot_nt(normed, wi_ref[...]) + ib_ref[...]
        fg_all = dot_nt(normed, wf_ref[...]) + fb_ref[...]
        fg_all = jnp.minimum(fg_all, 0.0) - jnp.log(1.0 + jnp.exp(-jnp.abs(fg_all)))
        for h in range(heads):
            pre = column(pre_all, first + h)
            shifted = column(fg_all, first + h) + to_column(m_ref[h : h + 1, :], pad_rows)
            new_m = jnp.maximum(shifted, pre)
            newm_ref[h : h + 1, :] = to_row(new_m, rows)
            gate_rows.append((jnp.exp(shifted - new_m), jnp.exp(pre - new_m) * dk**-0.5))
    row_ids = lax.broadcasted_iota(jnp.int32, (pad_rows, dk), 0)
    per_head = []
    with scope("queries"):
        finish(q_loads)
        queries = dot(normed, wq_ref[...]).astype(BF16).astype(F32)
        keys = dot(normed, wk_ref[...]).astype(BF16).astype(F32)
        for h in range(heads):
            forget, inflow = gate_rows[h]
            q = queries[:, h * dk : (h + 1) * dk]
            k = keys[:, h * dk : (h + 1) * dk] * inflow
            new_n = forget * padded(n_ref[:, h, :], pad_rows) + k
            newn_ref[:, h, :] = new_n[:rows]
            denom = jnp.maximum(jnp.abs(jnp.sum(q * new_n, axis=1, keepdims=True)), 1.0)
            inner = jnp.sum(q * k, axis=1, keepdims=True)
            wide = jnp.concatenate([jnp.where(row_ids == t, q, 0.0) for t in range(rows)], axis=1)
            per_head.append((forget, k, wide.astype(BF16), inner / denom, forget / denom))
    with scope("waits"):
        finish(v_loads)
        pltpu.make_async_copy(c_hbm, c_buf, load_sem.at[3]).wait()
    with scope("readout"):
        values = dot(normed, wv_ref[...]).astype(BF16).astype(F32)
        outs = []
        for h in range(heads):
            _, _, wide, inner, forget = per_head[h]
            read = dot(wide, c_buf[:, h].reshape(rows * dk, dv).astype(BF16))
            outs.append(forget * read + inner * values[:, h * dv : (h + 1) * dv])
        head_out = jnp.concatenate(outs, axis=1).astype(BF16)
    with scope("mix"):
        finish(mix_loads)
        part = dot(head_out, mix_buf[...]).astype(BF16).astype(F32)
        part_send[...] = pack(part, rows).astype(BF16)
    start(dense_loads)
    on_main(lambda: start(expert_loads))
    with scope("barrier"):
        pl.semaphore_wait(barrier, count)

    def mix_copy(dy):
        return remote(
            part_send, mixed.at[dy - 1], mix_s.at[dy - 1], mix_r.at[dy - 1], device(here, c, dy, 1)
        )

    for dy in other_planes:
        send(mix_copy(dy))

    def expert_copies(core, pieces=1):
        copies = []
        for i, (src, dst) in enumerate(((eg_hbm, eg), (eu_hbm, eu), (ed_hbm, ed))):
            size = src.shape[1] // pieces
            for piece in range(pieces):
                part_rows = pl.ds(piece * size, size)
                copies.append(
                    remote(
                        src.at[0, part_rows],
                        dst.at[core, part_rows],
                        e_s.at[core, i],
                        e_r.at[core, i],
                        device(here, main, 0, 1),
                    )
                )
        return copies

    on_side(lambda: start(expert_copies(c, PIECES)))

    with scope("routes"):
        scale = scale_ref[...].astype(F32)
        route_weight = scale / jnp.sum(scale, axis=0, keepdims=True)
        experts = own_w.shape[0] * nc
        ids = lax.broadcasted_iota(jnp.int32, (experts, rows), 0)
        table = jnp.zeros((experts, rows), F32)
        for k in range(routes_ref.shape[0]):
            table = table + jnp.where(ids == routes_ref[k : k + 1, :], route_weight[k : k + 1, :], 0.0)
        table = jnp.concatenate([table, jnp.zeros((experts, own_w.shape[2] - rows), F32)], axis=1)
        for e in range(experts):
            own_w[e // nc, e % nc : e % nc + 1, :] = table[e : e + 1, :]

        def w_copy(dz, dx):
            there = place(dz, dx, 1)
            return remote(
                own_w.at[there],
                weights.at[layer, slot(dz, dx)],
                w_s.at[0],
                w_r.at[layer],
                device(there, main, 0, 1),
            )

        for dz, dx in other_places:
            w_copy(dz, dx).start()
        on_side(lambda: w_copy(0, 0).start())

        @on_main
        def _():
            weights[0, 0] = own_w[here]

    with scope("ywait"):
        total = part
        for dy in other_planes:
            mix_copy(dy).wait_recv()
            total = total + unpack(mixed[dy - 1].astype(F32), rows)
    with scope("norm2"):
        residual = tokens + total.astype(BF16).astype(F32)
        ffn_f32 = rms_scaled(residual, fgain_ref[...])
        ffn_in = ffn_f32.astype(BF16)
        block_send[...] = pack(ffn_in.astype(F32), rows).astype(BF16)

        @on_main
        def _():
            inputs_ref[0, :pad_rows] = ffn_in

    def g_copy(dz, dx, there):
        return remote(
            block_send, blocks.at[layer, slot(dz, dx)], g_s.at[0], g_r.at[layer], device(there, main, 0, 1)
        )

    for step in far_first(1):
        g_copy(*step).start()
    on_side(lambda: g_copy(0, 0, here).start())

    def d_copy(dy):
        return remote(
            dense_send.at[dy - 1],
            dense_ref.at[dy - 1],
            d_s.at[dy - 1],
            d_r.at[dy - 1],
            device(here, c, dy, -1),
        )

    with scope("dense"):
        finish(dense_loads)
        dense_hidden = (jax.nn.silu(dot(ffn_in, dg[...])) * dot(ffn_in, du[...])).astype(BF16)
        wb = wb_ref[...].astype(F32)
        lanes = wb.shape[1]
        wide_in = ffn_in.astype(F32)
        branch = jnp.zeros((pad_rows, lanes), F32)
        for i in range(wb.shape[0]):
            branch = branch + wide_in[:, i * lanes : (i + 1) * lanes] * wb[i : i + 1, :]
        branch = jax.nn.sigmoid(jnp.sum(branch, axis=1, keepdims=True))

        def dense_part(dy):
            cols = pl.ds(pl.multiple_of(plane(dy, -1) * cw, cw), cw)
            return dot(dense_hidden, dd[:, cols]) * branch

        dense = [dense_part(dy) for dy in range(ntp)]
        for dy in other_planes:
            dense_send[dy - 1] = pack(dense[dy], rows).astype(BF16)
            send(d_copy(dy))
        own = dense[0]
        for j in range(ntp):
            own = own + jnp.where(tp == j, residual[:, j * cw : (j + 1) * cw], 0.0)

    with scope("newc"):
        for h in range(heads):
            forget, k = per_head[h][:2]
            v = values[:, h * dv : (h + 1) * dv]
            k_t = k.T
            for t in range(rows):
                newc_ref[t, h] = forget[t : t + 1] * c_buf[t, h] + k_t[:, t : t + 1] * v[t : t + 1]

    mine = tp * count_places + here

    def run_experts(core):
        index = main - core
        skip = 1 if core == main else 0
        with scope(f"factor{core}"):
            whole(weights.at[index, skip:], w_r.at[index]).wait_recv()
            factors = [
                jnp.concatenate(
                    [
                        to_column(weights[index, k, expert : expert + 1, :], pad_rows)
                        for k in range(count_places)
                    ],
                    axis=0,
                )
                for expert in range(nc)
            ]
        with scope(f"gwait{core}"):
            whole(blocks.at[index, skip:], g_r.at[index]).wait_recv()
        with scope(f"inputs{core}"):
            for k in range(skip, count_places):
                block = blocks[index, k].astype(F32)
                inputs_ref[index, k * pad_rows : (k + 1) * pad_rows] = unpack(block, rows).astype(BF16)
        hidden = [None] * nc
        for expert in range(nc - 1, -1, -1):
            if core == main:
                with scope("wwait"):
                    if expert == main:
                        finish(expert_loads)
                    else:
                        for copy in expert_copies(expert)[:2]:
                            copy.wait_recv()
            with scope(f"expert{core}"):
                inputs = inputs_ref[index]
                gate = jnp.minimum(dot(inputs, eg[expert]), CLAMP_LIMIT)
                up = jnp.clip(dot(inputs, eu[expert]), -CLAMP_LIMIT, CLAMP_LIMIT)
                act = gate * jax.nn.sigmoid(SWISH_ALPHA * gate) * (up + 1.0)
                hidden[expert] = (act * factors[expert]).astype(BF16)
        if core == main:
            with scope("wwait"):
                for expert in range(main):
                    expert_copies(expert)[2].wait_recv()
        for to in range(ntp):
            base = (index * ntp + to) * count_places
            with scope(f"down{core}"):
                cols = pl.ds(to * cw, cw)
                result = dot(hidden[0], ed[0, :, cols])
                for expert in range(1, nc):
                    result = result + dot(hidden[expert], ed[expert, :, cols])
                for k in range(count_places):
                    value = result[k * pad_rows : (k + 1) * pad_rows]
                    ret_send[base + k] = pack(value, rows).astype(BF16)
                for there in range(count_places):
                    dz = step_between(there // nx, z, nz)
                    dx = step_between(there % nx, x, nx)
                    copy = remote(
                        ret_send.at[base + slot(dz, dx)],
                        ret.at[mine],
                        r_s.at[0],
                        r_r.at[0],
                        {"ep": there * nc + core, "tp": to},
                    )
                    if core == main:
                        pl.when(mine != to * count_places + there)(copy.start)
                    else:
                        copy.start()
                if core == main:

                    @pl.when(tp == to)
                    def _():
                        ret[mine] = ret_send[base]

    @on_main
    def _():
        for core in range(main, -1, -1):
            run_experts(core)

    with scope("final"):
        for dy in other_planes:
            d_copy(dy).wait_recv()
        on_main(lambda: whole(ret.at[1:], r_r.at[0]).wait_recv())
        on_side(lambda: whole(ret, r_r.at[0]).wait_recv())
        total = ret[0].astype(F32)
        for i in range(1, ret.shape[0]):
            total = total + ret[i].astype(F32)
        for dy in other_planes:
            total = total + dense_ref[dy - 1].astype(F32)
        own = own + unpack(total, rows)
        out_ref[...] = own[:rows].astype(BF16)
    with scope("sendwait"):
        for copy in pending:
            copy.wait_send()

        @on_main
        def _():
            whole(weights.at[0, 1:], w_s.at[0]).wait_send()
            whole(blocks.at[0, 1:], g_s.at[0]).wait_send()
            whole(ret_send.at[1:], r_s.at[0]).wait_send()

        @on_side
        def _():
            whole(weights.at[0], w_s.at[0]).wait_send()
            whole(blocks.at[0], g_s.at[0]).wait_send()
            for copy in expert_copies(c):
                copy.wait_send()


def store_kernel(out_v, c_v, n_v, m_v, out_h, c_h, n_h, m_h, sem):
    copies = [
        pltpu.make_async_copy(src, dst, sem.at[0])
        for src, dst in ((out_v, out_h), (n_v, n_h), (m_v, m_h))
    ]
    states = [pltpu.make_async_copy(c_v.at[t], c_h.at[t], sem.at[1]) for t in range(c_v.shape[0])]
    for copy in copies + states:
        copy.start()
    for copy in copies:
        copy.wait()
    pltpu.make_async_copy(c_v, c_h, sem.at[1]).wait()


def local(
    sizes,
    tokens,
    norm_gain,
    w_query,
    w_key,
    w_value,
    w_input_gate,
    w_forget_gate,
    input_bias,
    forget_bias,
    state_c,
    state_n,
    state_m,
    w_mixer_out,
    ffn_gain,
    routes,
    route_scale,
    w_expert_gate,
    w_expert_up,
    w_expert_down,
    w_dense_gate,
    w_dense_up,
    w_dense_down,
    w_branch_gate,
):
    nz, nx, nc, ntp = sizes
    rows, width = tokens.shape
    pad_rows = -(-rows // 16) * 16
    cw = width // ntp
    vmem = pl.BlockSpec(memory_space=pltpu.VMEM)
    hbm = pl.BlockSpec(memory_space=pl.ANY)
    dma = pltpu.SemaphoreType.DMA
    wide_block = block_shape(rows, pad_rows, width)
    slim_block = block_shape(rows, pad_rows, cw)
    planes = max(1, ntp - 1)
    outs = pl.pallas_call(
        functools.partial(layer_kernel, sizes),
        name="layer",
        out_shape=(
            pltpu.VMEM((rows, cw), BF16),
            pltpu.VMEM(state_c.shape, F32),
            pltpu.VMEM(state_n.shape, F32),
            pltpu.VMEM(state_m.shape[::-1], F32),
        ),
        in_specs=[hbm] * 23,
        out_specs=(vmem,) * 4,
        scratch_shapes=[
            pltpu.VMEM(tokens.shape, BF16),
            pltpu.VMEM((1, width), F32),
            pltpu.VMEM(w_input_gate.shape[::-1], BF16),
            pltpu.VMEM(w_forget_gate.shape[::-1], BF16),
            pltpu.VMEM((1, input_bias.shape[0]), F32),
            pltpu.VMEM((1, forget_bias.shape[0]), F32),
            pltpu.VMEM(state_m.shape[::-1], F32),
            pltpu.VMEM(state_n.shape, F32),
            pltpu.VMEM(w_query.shape, BF16),
            pltpu.VMEM(w_key.shape, BF16),
            pltpu.VMEM(w_value.shape, BF16),
            pltpu.VMEM(state_c.shape, F32),
            pltpu.VMEM(w_mixer_out.shape, BF16),
            pltpu.VMEM((1, width), F32),
            pltpu.VMEM(routes.shape[::-1], jnp.int32),
            pltpu.VMEM(route_scale.shape[::-1], BF16),
            pltpu.VMEM((width // 128, 128), BF16),
            pltpu.VMEM(w_dense_gate.shape, BF16),
            pltpu.VMEM(w_dense_up.shape, BF16),
            pltpu.VMEM(w_dense_down.shape, BF16),
            pltpu.VMEM((nc,) + w_expert_gate.shape[1:], BF16),
            pltpu.VMEM((nc,) + w_expert_up.shape[1:], BF16),
            pltpu.VMEM((nc,) + w_expert_down.shape[1:], BF16),
            pltpu.VMEM(wide_block, BF16),
            pltpu.VMEM((planes,) + wide_block, BF16),
            pltpu.VMEM((nz * nx, nc, 128), F32),
            pltpu.VMEM((nc, nz * nx, nc, 128), F32),
            pltpu.VMEM(wide_block, BF16),
            pltpu.VMEM((nc, nz * nx) + wide_block, BF16),
            pltpu.VMEM((nc, nz * nx * pad_rows, width), BF16),
            pltpu.VMEM((planes,) + slim_block, BF16),
            pltpu.VMEM((planes,) + slim_block, BF16),
            pltpu.VMEM((nc * ntp * nz * nx,) + slim_block, BF16),
            pltpu.VMEM((ntp * nz * nx,) + slim_block, BF16),
            dma((8,)),
            dma((planes,)),
            dma((planes,)),
            dma((1,)),
            dma((nc,)),
            dma((1,)),
            dma((nc,)),
            dma((max(1, nc - 1), 3)),
            dma((max(1, nc - 1), 3)),
            dma((planes,)),
            dma((planes,)),
            dma((1,)),
            dma((1,)),
        ],
        compiler_params=pltpu.CompilerParams(
            vmem_limit_bytes=VMEM_LIMIT, collective_id=0, has_side_effects=True
        ),
    )(
        tokens,
        norm_gain.reshape(1, width),
        w_input_gate.T,
        w_forget_gate.T,
        input_bias.reshape(1, -1),
        forget_bias.reshape(1, -1),
        state_m.T,
        state_n,
        w_query,
        w_key,
        w_value,
        state_c,
        w_mixer_out,
        ffn_gain.reshape(1, width),
        routes.T,
        route_scale.T,
        w_branch_gate.reshape(width // 128, 128),
        w_dense_gate,
        w_dense_up,
        w_dense_down,
        w_expert_gate,
        w_expert_up,
        w_expert_down,
    )
    output, new_c, new_n, new_m = pl.pallas_call(
        store_kernel,
        name="store",
        out_shape=(
            jax.ShapeDtypeStruct((rows, cw), BF16),
            jax.ShapeDtypeStruct(state_c.shape, F32),
            jax.ShapeDtypeStruct(state_n.shape, F32),
            jax.ShapeDtypeStruct(state_m.shape[::-1], F32),
        ),
        in_specs=[vmem] * 4,
        out_specs=(hbm,) * 4,
        scratch_shapes=[dma((2,))],
        compiler_params=pltpu.CompilerParams(vmem_limit_bytes=1024 * 1024),
    )(*outs)
    return (output, new_c, new_n, new_m.T)


def solution(mesh):
    n_ep, n_tp = mesh.shape["ep"], mesh.shape["tp"]
    n_core = 2 if n_ep % 2 == 0 else 1
    n_x = n_tp if n_ep % (n_core * n_tp) == 0 else 1
    sizes = (n_ep // (n_core * n_x), n_x, n_core, n_tp)
    in_specs = (
        P("ep", None),
        P(),
        P(None, "tp"),
        P(None, "tp"),
        P(None, "tp"),
        P(),
        P(),
        P(),
        P(),
        P("ep", "tp", None, None),
        P("ep", "tp", None),
        P("ep", "tp"),
        P("tp", None),
        P(),
        P("ep", None),
        P("ep", None),
        P("ep", None, "tp"),
        P("ep", None, "tp"),
        P("ep", "tp", None),
        P(None, "tp"),
        P(None, "tp"),
        P("tp", None),
        P(),
    )
    out_specs = (P("ep", "tp"), P("ep", "tp", None, None), P("ep", "tp", None), P("ep", "tp"))
    return jax.shard_map(
        functools.partial(local, sizes),
        mesh=mesh,
        in_specs=in_specs,
        out_specs=out_specs,
        check_vma=False,
    )
```

```python
import functools

import jax
import jax.numpy as jnp
from jax import lax
from jax.experimental import pallas as pl
from jax.experimental.pallas import tpu as pltpu
from jax.sharding import PartitionSpec as P

EPSILON = 1e-06
CLAMP_LIMIT = 7.0
SWISH_ALPHA = 1.702
MESH = pl.DeviceIdType.MESH
F32 = jnp.float32
BF16 = jnp.bfloat16
VMEM_LIMIT = 60000 * 1024
PIECES = 4
scope = jax.named_scope


def padded(values, rows):
    extra = rows - values.shape[0]
    if extra == 0:
        return values
    return jnp.concatenate([values, jnp.zeros((extra, values.shape[1]), values.dtype)], axis=0)


def dot(left, right):
    return jnp.dot(left, right, preferred_element_type=F32)


def dot_nt(left, right):
    return lax.dot_general(left, right, (((1,), (1,)), ((), ())), preferred_element_type=F32)


def rms_scaled(values, gain):
    scale = lax.rsqrt(jnp.mean(values * values, axis=-1, keepdims=True) + EPSILON)
    return values * scale * gain


def to_column(row, rows):
    shape = (rows, row.shape[1])
    same = lax.broadcasted_iota(jnp.int32, shape, 0) == lax.broadcasted_iota(jnp.int32, shape, 1)
    return jnp.sum(jnp.where(same, row, 0.0), axis=1, keepdims=True)


def to_row(col, lanes):
    shape = (col.shape[0], lanes)
    same = lax.broadcasted_iota(jnp.int32, shape, 0) == lax.broadcasted_iota(jnp.int32, shape, 1)
    return jnp.sum(jnp.where(same, col, 0.0), axis=0, keepdims=True)


def column(values, index):
    lanes = lax.broadcasted_iota(jnp.int32, values.shape, 1)
    return jnp.sum(jnp.where(lanes == index, values, 0.0), axis=1, keepdims=True)


def dense_rows(rows):
    return 8 < rows <= 12


def block_shape(rows, pad_rows, width):
    return (8, width + width // 2) if dense_rows(rows) else (pad_rows, width)


def pack(values, rows):
    if not dense_rows(rows):
        return values
    half = values.shape[1] // 2
    low, high = values[8:16, :half], values[8:16, half:]
    top = lax.broadcasted_iota(jnp.int32, low.shape, 0) < 4
    return jnp.concatenate([values[:8], jnp.where(top, low, pltpu.roll(high, 4, 0))], axis=1)


def unpack(block, rows):
    if not dense_rows(rows):
        return block
    width = block.shape[1] // 3 * 2
    tail = block[:, width:]
    return jnp.concatenate(
        [block[:, :width], jnp.concatenate([tail, pltpu.roll(tail, 4, 0)], axis=1)], axis=0
    )


def partner(index, step, size, sign):
    if size & (size - 1):
        return lax.rem(index + sign * step + size, size)
    bit = 1
    while bit < size:
        if step & bit:
            index = index + bit * (1 - 2 * lax.rem(lax.div(index, bit), 2))
        bit *= 2
    return index


def step_between(a, b, size):
    if size & (size - 1):
        return lax.rem(b - a + size, size)
    step, bit = 0, 1
    while bit < size:
        step = step + bit * lax.rem(lax.div(a, bit) + lax.div(b, bit), 2)
        bit *= 2
    return step


def layer_kernel(
    sizes,
    tokens_hbm,
    gain_hbm,
    wi_hbm,
    wf_hbm,
    ib_hbm,
    fb_hbm,
    m_hbm,
    n_hbm,
    wq_hbm,
    wk_hbm,
    wv_hbm,
    c_hbm,
    mix_hbm,
    fgain_hbm,
    routes_hbm,
    scale_hbm,
    wb_hbm,
    dg_hbm,
    du_hbm,
    dd_hbm,
    eg_hbm,
    eu_hbm,
    ed_hbm,
    out_ref,
    newc_ref,
    newn_ref,
    newm_ref,
    tokens_ref,
    gain_ref,
    wi_ref,
    wf_ref,
    ib_ref,
    fb_ref,
    m_ref,
    n_ref,
    wq_ref,
    wk_ref,
    wv_ref,
    c_buf,
    mix_buf,
    fgain_ref,
    routes_ref,
    scale_ref,
    wb_ref,
    dg,
    du,
    dd,
    eg,
    eu,
    ed,
    part_send,
    mixed,
    own_w,
    weights,
    block_send,
    blocks,
    inputs_ref,
    dense_send,
    dense_ref,
    ret_send,
    ret,
    load_sem,
    mix_s,
    mix_r,
    w_s,
    w_r,
    g_s,
    g_r,
    e_s,
    e_r,
    d_s,
    d_r,
    r_s,
    r_r,
):
    nz, nx, nc, ntp = sizes
    ep = lax.axis_index("ep")
    tp = lax.axis_index("tp")
    c = lax.rem(ep, nc)
    x = lax.rem(lax.div(ep, nc), nx)
    z = lax.div(ep, nc * nx)
    rows, width = tokens_ref.shape
    pad_rows = inputs_ref.shape[1] // (nz * nx)
    heads = m_ref.shape[0]
    dk, dv = c_buf.shape[2], c_buf.shape[3]
    cw = width // ntp
    first = tp * heads
    main = nc - 1
    is_main = lax.div(c + 1, nc)
    layer = main - c
    count_places = nz * nx

    def on_main(body):
        return body() if nc == 1 else pl.when(c == main)(body)

    def on_side(body):
        return None if nc == 1 else pl.when(c != main)(body)

    def place(dz, dx, sign):
        return partner(z, dz, nz, sign) * nx + partner(x, dx, nx, sign)

    def plane(dy, sign):
        return partner(tp, dy, ntp, sign)

    def device(there, core, dy, sign):
        return {"ep": there * nc + core, "tp": plane(dy, sign)}

    def remote(src, dst, send, recv, device):
        return pltpu.make_async_remote_copy(
            src_ref=src, dst_ref=dst, send_sem=send, recv_sem=recv, device_id=device, device_id_type=MESH
        )

    def slot(dz, dx, dy=0):
        return (dy * nz + dz) * nx + dx

    here = place(0, 0, 1)
    pending = []

    def send(copy):
        copy.start()
        pending.append(copy)

    def whole(ref, sem):
        return remote(ref, ref, sem, sem, device(place(nz - 1, nx - 1, 1), c, ntp - 1, 1))

    def far_first(sign):
        steps = [(dz, dx) for dz in range(nz) for dx in range(nx)][1:]
        steps.sort(key=lambda step: -min(step[0], nz - step[0]) * nx - step[1])
        return [(dz, dx, place(dz, dx, sign)) for dz, dx in steps]

    places = [(dz, dx) for dz in range(nz - 1, -1, -1) for dx in range(nx - 1, -1, -1)]
    other_places = places[:-1]
    other_planes = list(range(1, ntp))

    def greet():
        barrier = pltpu.get_barrier_semaphore()

        def signal(there):
            pl.semaphore_signal(barrier, inc=1, device_id=there, device_id_type=MESH)

        for dy in other_planes:
            signal(device(here, c, dy, 1))

        @on_main
        def _():
            for dz, dx in places:
                for core in range(nc):
                    if (dz, dx, core) != (0, 0, main):
                        signal(device(place(dz, dx, 1), core, 0, 1))

        return barrier, len(other_planes) + count_places - is_main

    def group(index, *pairs):
        return [pltpu.make_async_copy(src, dst, load_sem.at[index]) for src, dst in pairs]

    first_loads = group(0, (tokens_hbm, tokens_ref), (gain_hbm, gain_ref))
    gate_loads = group(
        1,
        (wi_hbm, wi_ref),
        (wf_hbm, wf_ref),
        (ib_hbm, ib_ref),
        (fb_hbm, fb_ref),
        (m_hbm, m_ref),
        (n_hbm, n_ref),
    )
    q_loads = group(2, (wq_hbm, wq_ref), (wk_hbm, wk_ref))
    v_loads = group(7, (wv_hbm, wv_ref))
    c_loads = group(3, *((c_hbm.at[t], c_buf.at[t]) for t in range(rows)))
    mix_loads = group(
        4, (mix_hbm, mix_buf), (routes_hbm, routes_ref), (scale_hbm, scale_ref), (fgain_hbm, fgain_ref)
    )
    dense_loads = group(5, (wb_hbm, wb_ref), (dg_hbm, dg), (du_hbm, du), (dd_hbm, dd))
    expert_loads = group(
        6, (eg_hbm.at[0], eg.at[main]), (eu_hbm.at[0], eu.at[main]), (ed_hbm.at[0], ed.at[main])
    )

    def start(*groups):
        for copies in groups:
            for copy in copies:
                copy.start()

    def finish(copies):
        for copy in copies:
            copy.wait()

    start(first_loads)
    barrier, count = greet()
    start(gate_loads, q_loads, v_loads, c_loads, mix_loads)

    with scope("norm"):
        finish(first_loads)
        tokens = padded(tokens_ref[...].astype(F32), pad_rows)
        normed = rms_scaled(tokens, gain_ref[...]).astype(BF16)
    gate_rows = []
    with scope("gates"):
        finish(gate_loads)
        pre_all = dot_nt(normed, wi_ref[...]) + ib_ref[...]
        fg_all = dot_nt(normed, wf_ref[...]) + fb_ref[...]
        fg_all = jnp.minimum(fg_all, 0.0) - jnp.log(1.0 + jnp.exp(-jnp.abs(fg_all)))
        for h in range(heads):
            pre = column(pre_all, first + h)
            shifted = column(fg_all, first + h) + to_column(m_ref[h : h + 1, :], pad_rows)
            new_m = jnp.maximum(shifted, pre)
            newm_ref[h : h + 1, :] = to_row(new_m, rows)
            gate_rows.append((jnp.exp(shifted - new_m), jnp.exp(pre - new_m) * dk**-0.5))
    row_ids = lax.broadcasted_iota(jnp.int32, (pad_rows, dk), 0)
    per_head = []
    with scope("queries"):
        finish(q_loads)
        queries = dot(normed, wq_ref[...]).astype(BF16).astype(F32)
        keys = dot(normed, wk_ref[...]).astype(BF16).astype(F32)
        for h in range(heads):
            forget, inflow = gate_rows[h]
            q = queries[:, h * dk : (h + 1) * dk]
            k = keys[:, h * dk : (h + 1) * dk] * inflow
            new_n = forget * padded(n_ref[:, h, :], pad_rows) + k
            newn_ref[:, h, :] = new_n[:rows]
            denom = jnp.maximum(jnp.abs(jnp.sum(q * new_n, axis=1, keepdims=True)), 1.0)
            inner = jnp.sum(q * k, axis=1, keepdims=True)
            wide = jnp.concatenate([jnp.where(row_ids == t, q, 0.0) for t in range(rows)], axis=1)
            per_head.append((forget, k, wide.astype(BF16), inner / denom, forget / denom))
    with scope("waits"):
        finish(v_loads)
        pltpu.make_async_copy(c_hbm, c_buf, load_sem.at[3]).wait()
    with scope("readout"):
        values = dot(normed, wv_ref[...]).astype(BF16).astype(F32)
        outs = []
        for h in range(heads):
            _, _, wide, inner, forget = per_head[h]
            read = dot(wide, c_buf[:, h].reshape(rows * dk, dv).astype(BF16))
            outs.append(forget * read + inner * values[:, h * dv : (h + 1) * dv])
        head_out = jnp.concatenate(outs, axis=1).astype(BF16)
    with scope("mix"):
        finish(mix_loads)
        part = dot(head_out, mix_buf[...]).astype(BF16).astype(F32)
        part_send[...] = pack(part, rows).astype(BF16)
    start(dense_loads)
    on_main(lambda: start(expert_loads))
    with scope("barrier"):
        pl.semaphore_wait(barrier, count)

    def mix_copy(dy):
        return remote(
            part_send, mixed.at[dy - 1], mix_s.at[dy - 1], mix_r.at[dy - 1], device(here, c, dy, 1)
        )

    for dy in other_planes:
        send(mix_copy(dy))

    def expert_copies(core, pieces=1):
        copies = []
        for i, (src, dst) in enumerate(((eg_hbm, eg), (eu_hbm, eu), (ed_hbm, ed))):
            size = src.shape[1] // pieces
            for piece in range(pieces):
                part_rows = pl.ds(piece * size, size)
                copies.append(
                    remote(
                        src.at[0, part_rows],
                        dst.at[core, part_rows],
                        e_s.at[core, i],
                        e_r.at[core, i],
                        device(here, main, 0, 1),
                    )
                )
        return copies

    on_side(lambda: start(expert_copies(c, PIECES)))

    with scope("routes"):
        scale = scale_ref[...].astype(F32)
        route_weight = scale / jnp.sum(scale, axis=0, keepdims=True)
        experts = own_w.shape[0] * nc
        ids = lax.broadcasted_iota(jnp.int32, (experts, rows), 0)
        table = jnp.zeros((experts, rows), F32)
        for k in range(routes_ref.shape[0]):
            table = table + jnp.where(ids == routes_ref[k : k + 1, :], route_weight[k : k + 1, :], 0.0)
        table = jnp.concatenate([table, jnp.zeros((experts, own_w.shape[2] - rows), F32)], axis=1)
        for e in range(experts):
            own_w[e // nc, e % nc : e % nc + 1, :] = table[e : e + 1, :]

        def w_copy(dz, dx):
            there = place(dz, dx, 1)
            return remote(
                own_w.at[there],
                weights.at[layer, slot(dz, dx)],
                w_s.at[0],
                w_r.at[layer],
                device(there, main, 0, 1),
            )

        for dz, dx in other_places:
            w_copy(dz, dx).start()
        on_side(lambda: w_copy(0, 0).start())

        @on_main
        def _():
            weights[0, 0] = own_w[here]

    with scope("ywait"):
        total = part
        for dy in other_planes:
            mix_copy(dy).wait_recv()
            total = total + unpack(mixed[dy - 1].astype(F32), rows)
    with scope("norm2"):
        residual = tokens + total.astype(BF16).astype(F32)
        ffn_f32 = rms_scaled(residual, fgain_ref[...])
        ffn_in = ffn_f32.astype(BF16)
        block_send[...] = pack(ffn_in.astype(F32), rows).astype(BF16)

        @on_main
        def _():
            inputs_ref[0, :pad_rows] = ffn_in

    def g_copy(dz, dx, there):
        return remote(
            block_send, blocks.at[layer, slot(dz, dx)], g_s.at[0], g_r.at[layer], device(there, main, 0, 1)
        )

    for step in far_first(1):
        g_copy(*step).start()
    on_side(lambda: g_copy(0, 0, here).start())

    def d_copy(dy):
        return remote(
            dense_send.at[dy - 1],
            dense_ref.at[dy - 1],
            d_s.at[dy - 1],
            d_r.at[dy - 1],
            device(here, c, dy, -1),
        )

    with scope("dense"):
        finish(dense_loads)
        dense_hidden = (jax.nn.silu(dot(ffn_in, dg[...])) * dot(ffn_in, du[...])).astype(BF16)
        wb = wb_ref[...].astype(F32)
        lanes = wb.shape[1]
        wide_in = ffn_in.astype(F32)
        branch = jnp.zeros((pad_rows, lanes), F32)
        for i in range(wb.shape[0]):
            branch = branch + wide_in[:, i * lanes : (i + 1) * lanes] * wb[i : i + 1, :]
        branch = jax.nn.sigmoid(jnp.sum(branch, axis=1, keepdims=True))

        def dense_part(dy):
            cols = pl.ds(pl.multiple_of(plane(dy, -1) * cw, cw), cw)
            return dot(dense_hidden, dd[:, cols]) * branch

        dense = [dense_part(dy) for dy in range(ntp)]
        for dy in other_planes:
            dense_send[dy - 1] = pack(dense[dy], rows).astype(BF16)
            send(d_copy(dy))
        own = dense[0]
        for j in range(ntp):
            own = own + jnp.where(tp == j, residual[:, j * cw : (j + 1) * cw], 0.0)

    with scope("newc"):
        for h in range(heads):
            forget, k = per_head[h][:2]
            v = values[:, h * dv : (h + 1) * dv]
            k_t = k.T
            for t in range(rows):
                newc_ref[t, h] = forget[t : t + 1] * c_buf[t, h] + k_t[:, t : t + 1] * v[t : t + 1]

    mine = tp * count_places + here

    def run_experts(core):
        index = main - core
        skip = 1 if core == main else 0
        with scope(f"factor{core}"):
            whole(weights.at[index, skip:], w_r.at[index]).wait_recv()
            factors = [
                jnp.concatenate(
                    [
                        to_column(weights[index, k, expert : expert + 1, :], pad_rows)
                        for k in range(count_places)
                    ],
                    axis=0,
                )
                for expert in range(nc)
            ]
        with scope(f"gwait{core}"):
            whole(blocks.at[index, skip:], g_r.at[index]).wait_recv()
        with scope(f"inputs{core}"):
            for k in range(skip, count_places):
                block = blocks[index, k].astype(F32)
                inputs_ref[index, k * pad_rows : (k + 1) * pad_rows] = unpack(block, rows).astype(BF16)
        hidden = [None] * nc
        for expert in range(nc - 1, -1, -1):
            if core == main:
                with scope("wwait"):
                    if expert == main:
                        finish(expert_loads)
                    else:
                        for copy in expert_copies(expert)[:2]:
                            copy.wait_recv()
            with scope(f"expert{core}"):
                inputs = inputs_ref[index]
                gate = jnp.minimum(dot(inputs, eg[expert]), CLAMP_LIMIT)
                up = jnp.clip(dot(inputs, eu[expert]), -CLAMP_LIMIT, CLAMP_LIMIT)
                act = gate * jax.nn.sigmoid(SWISH_ALPHA * gate) * (up + 1.0)
                hidden[expert] = (act * factors[expert]).astype(BF16)
        if core == main:
            with scope("wwait"):
                for expert in range(main):
                    expert_copies(expert)[2].wait_recv()
        def leave(to, low, high):
            base = (index * ntp + to) * count_places
            for there in range(low, high):
                dz = step_between(there // nx, z, nz)
                dx = step_between(there % nx, x, nx)
                copy = remote(
                    ret_send.at[base + slot(dz, dx)],
                    ret.at[mine],
                    r_s.at[0],
                    r_r.at[0],
                    {"ep": there * nc + core, "tp": to},
                )
                if core == main:
                    pl.when(mine != to * count_places + there)(copy.start)
                else:
                    copy.start()

        half = count_places // 2
        for to in range(ntp):
            base = (index * ntp + to) * count_places
            with scope(f"down{core}"):
                cols = pl.ds(to * cw, cw)
                result = dot(hidden[0], ed[0, :, cols])
                for expert in range(1, nc):
                    result = result + dot(hidden[expert], ed[expert, :, cols])
                for k in range(count_places):
                    value = result[k * pad_rows : (k + 1) * pad_rows]
                    ret_send[base + k] = pack(value, rows).astype(BF16)
                leave(to, 0, half)
                if core == main:

                    @pl.when(tp == to)
                    def _():
                        ret[mine] = ret_send[base]

        far_ones = [functools.partial(leave, to, half, count_places) for to in range(ntp)]
        if core == main and main > 0:
            kept = len(far_ones) // 2
            held.extend(far_ones[kept:])
            far_ones = far_ones[:kept]
        else:
            far_ones = held + far_ones
        for far_one in far_ones:
            far_one()

    held = []

    @on_main
    def _():
        for core in range(main, -1, -1):
            run_experts(core)

    with scope("final"):
        for dy in other_planes:
            d_copy(dy).wait_recv()
        on_main(lambda: whole(ret.at[1:], r_r.at[0]).wait_recv())
        on_side(lambda: whole(ret, r_r.at[0]).wait_recv())
        total = ret[0].astype(F32)
        for i in range(1, ret.shape[0]):
            total = total + ret[i].astype(F32)
        for dy in other_planes:
            total = total + dense_ref[dy - 1].astype(F32)
        own = own + unpack(total, rows)
        out_ref[...] = own[:rows].astype(BF16)
    with scope("sendwait"):
        for copy in pending:
            copy.wait_send()

        @on_main
        def _():
            whole(weights.at[0, 1:], w_s.at[0]).wait_send()
            whole(blocks.at[0, 1:], g_s.at[0]).wait_send()
            whole(ret_send.at[1:], r_s.at[0]).wait_send()

        @on_side
        def _():
            whole(weights.at[0], w_s.at[0]).wait_send()
            whole(blocks.at[0], g_s.at[0]).wait_send()
            for copy in expert_copies(c):
                copy.wait_send()


def store_kernel(out_v, c_v, n_v, m_v, out_h, c_h, n_h, m_h, sem):
    copies = [
        pltpu.make_async_copy(src, dst, sem.at[0])
        for src, dst in ((out_v, out_h), (n_v, n_h), (m_v, m_h))
    ]
    states = [pltpu.make_async_copy(c_v.at[t], c_h.at[t], sem.at[1]) for t in range(c_v.shape[0])]
    for copy in copies + states:
        copy.start()
    for copy in copies:
        copy.wait()
    pltpu.make_async_copy(c_v, c_h, sem.at[1]).wait()


def local(
    sizes,
    tokens,
    norm_gain,
    w_query,
    w_key,
    w_value,
    w_input_gate,
    w_forget_gate,
    input_bias,
    forget_bias,
    state_c,
    state_n,
    state_m,
    w_mixer_out,
    ffn_gain,
    routes,
    route_scale,
    w_expert_gate,
    w_expert_up,
    w_expert_down,
    w_dense_gate,
    w_dense_up,
    w_dense_down,
    w_branch_gate,
):
    nz, nx, nc, ntp = sizes
    rows, width = tokens.shape
    pad_rows = -(-rows // 16) * 16
    cw = width // ntp
    vmem = pl.BlockSpec(memory_space=pltpu.VMEM)
    hbm = pl.BlockSpec(memory_space=pl.ANY)
    dma = pltpu.SemaphoreType.DMA
    wide_block = block_shape(rows, pad_rows, width)
    slim_block = block_shape(rows, pad_rows, cw)
    planes = max(1, ntp - 1)
    outs = pl.pallas_call(
        functools.partial(layer_kernel, sizes),
        name="layer",
        out_shape=(
            pltpu.VMEM((rows, cw), BF16),
            pltpu.VMEM(state_c.shape, F32),
            pltpu.VMEM(state_n.shape, F32),
            pltpu.VMEM(state_m.shape[::-1], F32),
        ),
        in_specs=[hbm] * 23,
        out_specs=(vmem,) * 4,
        scratch_shapes=[
            pltpu.VMEM(tokens.shape, BF16),
            pltpu.VMEM((1, width), F32),
            pltpu.VMEM(w_input_gate.shape[::-1], BF16),
            pltpu.VMEM(w_forget_gate.shape[::-1], BF16),
            pltpu.VMEM((1, input_bias.shape[0]), F32),
            pltpu.VMEM((1, forget_bias.shape[0]), F32),
            pltpu.VMEM(state_m.shape[::-1], F32),
            pltpu.VMEM(state_n.shape, F32),
            pltpu.VMEM(w_query.shape, BF16),
            pltpu.VMEM(w_key.shape, BF16),
            pltpu.VMEM(w_value.shape, BF16),
            pltpu.VMEM(state_c.shape, F32),
            pltpu.VMEM(w_mixer_out.shape, BF16),
            pltpu.VMEM((1, width), F32),
            pltpu.VMEM(routes.shape[::-1], jnp.int32),
            pltpu.VMEM(route_scale.shape[::-1], BF16),
            pltpu.VMEM((width // 128, 128), BF16),
            pltpu.VMEM(w_dense_gate.shape, BF16),
            pltpu.VMEM(w_dense_up.shape, BF16),
            pltpu.VMEM(w_dense_down.shape, BF16),
            pltpu.VMEM((nc,) + w_expert_gate.shape[1:], BF16),
            pltpu.VMEM((nc,) + w_expert_up.shape[1:], BF16),
            pltpu.VMEM((nc,) + w_expert_down.shape[1:], BF16),
            pltpu.VMEM(wide_block, BF16),
            pltpu.VMEM((planes,) + wide_block, BF16),
            pltpu.VMEM((nz * nx, nc, 128), F32),
            pltpu.VMEM((nc, nz * nx, nc, 128), F32),
            pltpu.VMEM(wide_block, BF16),
            pltpu.VMEM((nc, nz * nx) + wide_block, BF16),
            pltpu.VMEM((nc, nz * nx * pad_rows, width), BF16),
            pltpu.VMEM((planes,) + slim_block, BF16),
            pltpu.VMEM((planes,) + slim_block, BF16),
            pltpu.VMEM((nc * ntp * nz * nx,) + slim_block, BF16),
            pltpu.VMEM((ntp * nz * nx,) + slim_block, BF16),
            dma((8,)),
            dma((planes,)),
            dma((planes,)),
            dma((1,)),
            dma((nc,)),
            dma((1,)),
            dma((nc,)),
            dma((max(1, nc - 1), 3)),
            dma((max(1, nc - 1), 3)),
            dma((planes,)),
            dma((planes,)),
            dma((1,)),
            dma((1,)),
        ],
        compiler_params=pltpu.CompilerParams(
            vmem_limit_bytes=VMEM_LIMIT, collective_id=0, has_side_effects=True
        ),
    )(
        tokens,
        norm_gain.reshape(1, width),
        w_input_gate.T,
        w_forget_gate.T,
        input_bias.reshape(1, -1),
        forget_bias.reshape(1, -1),
        state_m.T,
        state_n,
        w_query,
        w_key,
        w_value,
        state_c,
        w_mixer_out,
        ffn_gain.reshape(1, width),
        routes.T,
        route_scale.T,
        w_branch_gate.reshape(width // 128, 128),
        w_dense_gate,
        w_dense_up,
        w_dense_down,
        w_expert_gate,
        w_expert_up,
        w_expert_down,
    )
    output, new_c, new_n, new_m = pl.pallas_call(
        store_kernel,
        name="store",
        out_shape=(
            jax.ShapeDtypeStruct((rows, cw), BF16),
            jax.ShapeDtypeStruct(state_c.shape, F32),
            jax.ShapeDtypeStruct(state_n.shape, F32),
            jax.ShapeDtypeStruct(state_m.shape[::-1], F32),
        ),
        in_specs=[vmem] * 4,
        out_specs=(hbm,) * 4,
        scratch_shapes=[dma((2,))],
        compiler_params=pltpu.CompilerParams(vmem_limit_bytes=1024 * 1024),
    )(*outs)
    return (output, new_c, new_n, new_m.T)


def solution(mesh):
    n_ep, n_tp = mesh.shape["ep"], mesh.shape["tp"]
    n_core = 2 if n_ep % 2 == 0 else 1
    n_x = n_tp if n_ep % (n_core * n_tp) == 0 else 1
    sizes = (n_ep // (n_core * n_x), n_x, n_core, n_tp)
    in_specs = (
        P("ep", None),
        P(),
        P(None, "tp"),
        P(None, "tp"),
        P(None, "tp"),
        P(),
        P(),
        P(),
        P(),
        P("ep", "tp", None, None),
        P("ep", "tp", None),
        P("ep", "tp"),
        P("tp", None),
        P(),
        P("ep", None),
        P("ep", None),
        P("ep", None, "tp"),
        P("ep", None, "tp"),
        P("ep", "tp", None),
        P(None, "tp"),
        P(None, "tp"),
        P("tp", None),
        P(),
    )
    out_specs = (P("ep", "tp"), P("ep", "tp", None, None), P("ep", "tp", None), P("ep", "tp"))
    return jax.shard_map(
        functools.partial(local, sizes),
        mesh=mesh,
        in_specs=in_specs,
        out_specs=out_specs,
        check_vma=False,
    )
```

```python
import functools

import jax
import jax.numpy as jnp
from jax import lax
from jax.experimental import pallas as pl
from jax.experimental.pallas import tpu as pltpu
from jax.sharding import PartitionSpec as P

EPSILON = 1e-06
CLAMP_LIMIT = 7.0
SWISH_ALPHA = 1.702
MESH = pl.DeviceIdType.MESH
F32 = jnp.float32
BF16 = jnp.bfloat16
VMEM_LIMIT = 60000 * 1024
PIECES = 4
scope = jax.named_scope


def padded(values, rows):
    extra = rows - values.shape[0]
    if extra == 0:
        return values
    return jnp.concatenate([values, jnp.zeros((extra, values.shape[1]), values.dtype)], axis=0)


def dot(left, right):
    return jnp.dot(left, right, preferred_element_type=F32)


def dot_nt(left, right):
    return lax.dot_general(left, right, (((1,), (1,)), ((), ())), preferred_element_type=F32)


def rms_scaled(values, gain):
    scale = lax.rsqrt(jnp.mean(values * values, axis=-1, keepdims=True) + EPSILON)
    return values * scale * gain


def to_column(row, rows):
    shape = (rows, row.shape[1])
    same = lax.broadcasted_iota(jnp.int32, shape, 0) == lax.broadcasted_iota(jnp.int32, shape, 1)
    return jnp.sum(jnp.where(same, row, 0.0), axis=1, keepdims=True)


def to_row(col, lanes):
    shape = (col.shape[0], lanes)
    same = lax.broadcasted_iota(jnp.int32, shape, 0) == lax.broadcasted_iota(jnp.int32, shape, 1)
    return jnp.sum(jnp.where(same, col, 0.0), axis=0, keepdims=True)


def column(values, index):
    lanes = lax.broadcasted_iota(jnp.int32, values.shape, 1)
    return jnp.sum(jnp.where(lanes == index, values, 0.0), axis=1, keepdims=True)


def dense_rows(rows):
    return 8 < rows <= 12


def block_shape(rows, pad_rows, width):
    return (8, width + width // 2) if dense_rows(rows) else (pad_rows, width)


def pack(values, rows):
    if not dense_rows(rows):
        return values
    half = values.shape[1] // 2
    low, high = values[8:16, :half], values[8:16, half:]
    top = lax.broadcasted_iota(jnp.int32, low.shape, 0) < 4
    return jnp.concatenate([values[:8], jnp.where(top, low, pltpu.roll(high, 4, 0))], axis=1)


def unpack(block, rows):
    if not dense_rows(rows):
        return block
    width = block.shape[1] // 3 * 2
    tail = block[:, width:]
    return jnp.concatenate(
        [block[:, :width], jnp.concatenate([tail, pltpu.roll(tail, 4, 0)], axis=1)], axis=0
    )


def partner(index, step, size, sign):
    if size & (size - 1):
        return lax.rem(index + sign * step + size, size)
    bit = 1
    while bit < size:
        if step & bit:
            index = index + bit * (1 - 2 * lax.rem(lax.div(index, bit), 2))
        bit *= 2
    return index


def step_between(a, b, size):
    if size & (size - 1):
        return lax.rem(b - a + size, size)
    step, bit = 0, 1
    while bit < size:
        step = step + bit * lax.rem(lax.div(a, bit) + lax.div(b, bit), 2)
        bit *= 2
    return step


def layer_kernel(
    sizes,
    tokens_hbm,
    gain_hbm,
    wi_hbm,
    wf_hbm,
    ib_hbm,
    fb_hbm,
    m_hbm,
    n_hbm,
    wq_hbm,
    wk_hbm,
    wv_hbm,
    c_hbm,
    mix_hbm,
    fgain_hbm,
    routes_hbm,
    scale_hbm,
    wb_hbm,
    dg_hbm,
    du_hbm,
    dd_hbm,
    eg_hbm,
    eu_hbm,
    ed_hbm,
    out_ref,
    newc_ref,
    newn_ref,
    newm_ref,
    tokens_ref,
    gain_ref,
    wi_ref,
    wf_ref,
    ib_ref,
    fb_ref,
    m_ref,
    n_ref,
    wq_ref,
    wk_ref,
    wv_ref,
    c_buf,
    mix_buf,
    fgain_ref,
    routes_ref,
    scale_ref,
    wb_ref,
    dg,
    du,
    dd,
    eg,
    eu,
    ed,
    part_send,
    mixed,
    own_w,
    weights,
    block_send,
    blocks,
    inputs_ref,
    dense_send,
    dense_ref,
    ret_send,
    ret,
    load_sem,
    mix_s,
    mix_r,
    w_s,
    w_r,
    g_s,
    g_r,
    e_s,
    e_r,
    d_s,
    d_r,
    r_s,
    r_r,
):
    nz, nx, nc, ntp = sizes
    ep = lax.axis_index("ep")
    tp = lax.axis_index("tp")
    c = lax.rem(ep, nc)
    x = lax.rem(lax.div(ep, nc), nx)
    z = lax.div(ep, nc * nx)
    rows, width = tokens_ref.shape
    pad_rows = inputs_ref.shape[1] // (nz * nx)
    heads = m_ref.shape[0]
    dk, dv = c_buf.shape[2], c_buf.shape[3]
    cw = width // ntp
    first = tp * heads
    main = nc - 1
    is_main = lax.div(c + 1, nc)
    layer = main - c
    count_places = nz * nx

    def on_main(body):
        return body() if nc == 1 else pl.when(c == main)(body)

    def on_side(body):
        return None if nc == 1 else pl.when(c != main)(body)

    def place(dz, dx, sign):
        return partner(z, dz, nz, sign) * nx + partner(x, dx, nx, sign)

    def plane(dy, sign):
        return partner(tp, dy, ntp, sign)

    def device(there, core, dy, sign):
        return {"ep": there * nc + core, "tp": plane(dy, sign)}

    def remote(src, dst, send, recv, device):
        return pltpu.make_async_remote_copy(
            src_ref=src, dst_ref=dst, send_sem=send, recv_sem=recv, device_id=device, device_id_type=MESH
        )

    def slot(dz, dx, dy=0):
        return (dy * nz + dz) * nx + dx

    here = place(0, 0, 1)
    pending = []

    def send(copy):
        copy.start()
        pending.append(copy)

    def whole(ref, sem):
        return remote(ref, ref, sem, sem, device(place(nz - 1, nx - 1, 1), c, ntp - 1, 1))

    def far_first(sign):
        steps = [(dz, dx) for dz in range(nz) for dx in range(nx)][1:]
        steps.sort(key=lambda step: -min(step[0], nz - step[0]) * nx - step[1])
        return [(dz, dx, place(dz, dx, sign)) for dz, dx in steps]

    places = [(dz, dx) for dz in range(nz - 1, -1, -1) for dx in range(nx - 1, -1, -1)]
    other_places = places[:-1]
    other_planes = list(range(1, ntp))

    def greet():
        barrier = pltpu.get_barrier_semaphore()

        def signal(there):
            pl.semaphore_signal(barrier, inc=1, device_id=there, device_id_type=MESH)

        for dy in other_planes:
            signal(device(here, c, dy, 1))

        @on_main
        def _():
            for dz, dx in places:
                for core in range(nc):
                    if (dz, dx, core) != (0, 0, main):
                        signal(device(place(dz, dx, 1), core, 0, 1))

        return barrier, len(other_planes) + count_places - is_main

    def group(index, *pairs):
        return [pltpu.make_async_copy(src, dst, load_sem.at[index]) for src, dst in pairs]

    first_loads = group(0, (tokens_hbm, tokens_ref), (gain_hbm, gain_ref))
    gate_loads = group(
        1,
        (wi_hbm, wi_ref),
        (wf_hbm, wf_ref),
        (ib_hbm, ib_ref),
        (fb_hbm, fb_ref),
        (m_hbm, m_ref),
        (n_hbm, n_ref),
    )
    q_loads = group(2, (wq_hbm, wq_ref), (wk_hbm, wk_ref))
    v_loads = group(7, (wv_hbm, wv_ref))
    c_loads = group(3, *((c_hbm.at[t], c_buf.at[t]) for t in range(rows)))
    mix_loads = group(
        4, (mix_hbm, mix_buf), (routes_hbm, routes_ref), (scale_hbm, scale_ref), (fgain_hbm, fgain_ref)
    )
    dense_loads = group(5, (wb_hbm, wb_ref), (dg_hbm, dg), (du_hbm, du), (dd_hbm, dd))
    expert_loads = group(
        6, (eg_hbm.at[0], eg.at[main]), (eu_hbm.at[0], eu.at[main]), (ed_hbm.at[0], ed.at[main])
    )

    def start(*groups):
        for copies in groups:
            for copy in copies:
                copy.start()

    def finish(copies):
        for copy in copies:
            copy.wait()

    start(first_loads)
    barrier, count = greet()
    start(gate_loads, q_loads, v_loads, c_loads, mix_loads)

    with scope("norm"):
        finish(first_loads)
        tokens = padded(tokens_ref[...].astype(F32), pad_rows)
        normed = rms_scaled(tokens, gain_ref[...]).astype(BF16)
    gate_rows = []
    with scope("gates"):
        finish(gate_loads)
        pre_all = dot_nt(normed, wi_ref[...]) + ib_ref[...]
        fg_all = dot_nt(normed, wf_ref[...]) + fb_ref[...]
        fg_all = jnp.minimum(fg_all, 0.0) - jnp.log(1.0 + jnp.exp(-jnp.abs(fg_all)))
        for h in range(heads):
            pre = column(pre_all, first + h)
            shifted = column(fg_all, first + h) + to_column(m_ref[h : h + 1, :], pad_rows)
            new_m = jnp.maximum(shifted, pre)
            newm_ref[h : h + 1, :] = to_row(new_m, rows)
            gate_rows.append((jnp.exp(shifted - new_m), jnp.exp(pre - new_m) * dk**-0.5))
    row_ids = lax.broadcasted_iota(jnp.int32, (pad_rows, dk), 0)
    per_head = []
    with scope("queries"):
        finish(q_loads)
        queries = dot(normed, wq_ref[...]).astype(BF16).astype(F32)
        keys = dot(normed, wk_ref[...]).astype(BF16).astype(F32)
        for h in range(heads):
            forget, inflow = gate_rows[h]
            q = queries[:, h * dk : (h + 1) * dk]
            k = keys[:, h * dk : (h + 1) * dk] * inflow
            new_n = forget * padded(n_ref[:, h, :], pad_rows) + k
            newn_ref[:, h, :] = new_n[:rows]
            denom = jnp.maximum(jnp.abs(jnp.sum(q * new_n, axis=1, keepdims=True)), 1.0)
            inner = jnp.sum(q * k, axis=1, keepdims=True)
            wide = jnp.concatenate([jnp.where(row_ids == t, q, 0.0) for t in range(rows)], axis=1)
            per_head.append((forget, k, wide.astype(BF16), inner / denom, forget / denom))
    with scope("waits"):
        finish(v_loads)
        pltpu.make_async_copy(c_hbm, c_buf, load_sem.at[3]).wait()
    with scope("readout"):
        values = dot(normed, wv_ref[...]).astype(BF16).astype(F32)
        outs = []
        for h in range(heads):
            _, _, wide, inner, forget = per_head[h]
            read = dot(wide, c_buf[:, h].reshape(rows * dk, dv).astype(BF16))
            outs.append(forget * read + inner * values[:, h * dv : (h + 1) * dv])
        head_out = jnp.concatenate(outs, axis=1).astype(BF16)
    with scope("mix"):
        finish(mix_loads)
        part = dot(head_out, mix_buf[...]).astype(BF16).astype(F32)
        part_send[...] = pack(part, rows).astype(BF16)
    start(dense_loads)
    on_main(lambda: start(expert_loads))
    with scope("barrier"):
        pl.semaphore_wait(barrier, count)

    def mix_copy(dy):
        return remote(
            part_send, mixed.at[dy - 1], mix_s.at[dy - 1], mix_r.at[dy - 1], device(here, c, dy, 1)
        )

    for dy in other_planes:
        send(mix_copy(dy))

    def expert_copies(core, pieces=1):
        copies = []
        for i, (src, dst) in enumerate(((eg_hbm, eg), (eu_hbm, eu), (ed_hbm, ed))):
            size = src.shape[1] // pieces
            for piece in range(pieces):
                part_rows = pl.ds(piece * size, size)
                copies.append(
                    remote(
                        src.at[0, part_rows],
                        dst.at[core, part_rows],
                        e_s.at[core, i],
                        e_r.at[core, i],
                        device(here, main, 0, 1),
                    )
                )
        return copies

    on_side(lambda: start(expert_copies(c, PIECES)))

    with scope("routes"):
        scale = scale_ref[...].astype(F32)
        route_weight = scale / jnp.sum(scale, axis=0, keepdims=True)
        experts = own_w.shape[0] * nc
        ids = lax.broadcasted_iota(jnp.int32, (experts, rows), 0)
        table = jnp.zeros((experts, rows), F32)
        for k in range(routes_ref.shape[0]):
            table = table + jnp.where(ids == routes_ref[k : k + 1, :], route_weight[k : k + 1, :], 0.0)
        table = jnp.concatenate([table, jnp.zeros((experts, own_w.shape[2] - rows), F32)], axis=1)
        for e in range(experts):
            own_w[e // nc, e % nc : e % nc + 1, :] = table[e : e + 1, :]

        def w_copy(dz, dx):
            there = place(dz, dx, 1)
            return remote(
                own_w.at[there],
                weights.at[layer, slot(dz, dx)],
                w_s.at[0],
                w_r.at[layer],
                device(there, main, 0, 1),
            )

        for dz, dx in other_places:
            w_copy(dz, dx).start()
        on_side(lambda: w_copy(0, 0).start())

        @on_main
        def _():
            weights[0, 0] = own_w[here]

    with scope("ywait"):
        total = part
        for dy in other_planes:
            mix_copy(dy).wait_recv()
            total = total + unpack(mixed[dy - 1].astype(F32), rows)
    with scope("norm2"):
        residual = tokens + total.astype(BF16).astype(F32)
        ffn_f32 = rms_scaled(residual, fgain_ref[...])
        ffn_in = ffn_f32.astype(BF16)
        block_send[...] = pack(ffn_in.astype(F32), rows).astype(BF16)

        @on_main
        def _():
            inputs_ref[0, :pad_rows] = ffn_in

    def g_copy(dz, dx, there):
        return remote(
            block_send, blocks.at[layer, slot(dz, dx)], g_s.at[0], g_r.at[layer], device(there, main, 0, 1)
        )

    for step in far_first(1):
        g_copy(*step).start()
    on_side(lambda: g_copy(0, 0, here).start())

    def d_copy(dy):
        return remote(
            dense_send.at[dy - 1],
            dense_ref.at[dy - 1],
            d_s.at[dy - 1],
            d_r.at[dy - 1],
            device(here, c, dy, -1),
        )

    with scope("dense"):
        finish(dense_loads)
        dense_hidden = (jax.nn.silu(dot(ffn_in, dg[...])) * dot(ffn_in, du[...])).astype(BF16)
        wb = wb_ref[...].astype(F32)
        lanes = wb.shape[1]
        wide_in = ffn_in.astype(F32)
        branch = jnp.zeros((pad_rows, lanes), F32)
        for i in range(wb.shape[0]):
            branch = branch + wide_in[:, i * lanes : (i + 1) * lanes] * wb[i : i + 1, :]
        branch = jax.nn.sigmoid(jnp.sum(branch, axis=1, keepdims=True))

        def dense_part(dy):
            cols = pl.ds(pl.multiple_of(plane(dy, -1) * cw, cw), cw)
            return dot(dense_hidden, dd[:, cols]) * branch

        dense = [dense_part(dy) for dy in range(ntp)]
        for dy in other_planes:
            dense_send[dy - 1] = pack(dense[dy], rows).astype(BF16)
            send(d_copy(dy))
        own = dense[0]
        for j in range(ntp):
            own = own + jnp.where(tp == j, residual[:, j * cw : (j + 1) * cw], 0.0)

    with scope("newc"):
        for h in range(heads):
            forget, k = per_head[h][:2]
            v = values[:, h * dv : (h + 1) * dv]
            k_t = k.T
            for t in range(rows):
                newc_ref[t, h] = forget[t : t + 1] * c_buf[t, h] + k_t[:, t : t + 1] * v[t : t + 1]

    mine = tp * count_places + here

    def run_experts(core):
        index = main - core
        skip = 1 if core == main else 0
        with scope(f"factor{core}"):
            whole(weights.at[index, skip:], w_r.at[index]).wait_recv()
            factors = [
                jnp.concatenate(
                    [
                        to_column(weights[index, k, expert : expert + 1, :], pad_rows)
                        for k in range(count_places)
                    ],
                    axis=0,
                )
                for expert in range(nc)
            ]
        with scope(f"gwait{core}"):
            whole(blocks.at[index, skip:], g_r.at[index]).wait_recv()
        with scope(f"inputs{core}"):
            for k in range(skip, count_places):
                block = blocks[index, k].astype(F32)
                inputs_ref[index, k * pad_rows : (k + 1) * pad_rows] = unpack(block, rows).astype(BF16)
        hidden = [None] * nc
        if core == main:
            with scope("wwait"):
                finish(expert_loads)
                for expert in range(main):
                    for copy in expert_copies(expert)[:2]:
                        copy.wait_recv()
        for expert in range(nc - 1, -1, -1):
            with scope(f"expert{core}"):
                inputs = inputs_ref[index]
                gate = jnp.minimum(dot(inputs, eg[expert]), CLAMP_LIMIT)
                up = jnp.clip(dot(inputs, eu[expert]), -CLAMP_LIMIT, CLAMP_LIMIT)
                act = gate * jax.nn.sigmoid(SWISH_ALPHA * gate) * (up + 1.0)
                hidden[expert] = (act * factors[expert]).astype(BF16)
        if core == main:
            with scope("wwait"):
                for expert in range(main):
                    expert_copies(expert)[2].wait_recv()
        def leave(to, low, high):
            base = (index * ntp + to) * count_places
            for there in range(low, high):
                dz = step_between(there // nx, z, nz)
                dx = step_between(there % nx, x, nx)
                copy = remote(
                    ret_send.at[base + slot(dz, dx)],
                    ret.at[mine],
                    r_s.at[0],
                    r_r.at[0],
                    {"ep": there * nc + core, "tp": to},
                )
                if core == main:
                    pl.when(mine != to * count_places + there)(copy.start)
                else:
                    copy.start()

        half = count_places // 2
        for to in range(ntp):
            base = (index * ntp + to) * count_places
            with scope(f"down{core}"):
                cols = pl.ds(to * cw, cw)
                result = dot(hidden[0], ed[0, :, cols])
                for expert in range(1, nc):
                    result = result + dot(hidden[expert], ed[expert, :, cols])
                for k in range(count_places):
                    value = result[k * pad_rows : (k + 1) * pad_rows]
                    ret_send[base + k] = pack(value, rows).astype(BF16)
                leave(to, 0, half)
                if core == main:

                    @pl.when(tp == to)
                    def _():
                        ret[mine] = ret_send[base]

        far_ones = [functools.partial(leave, to, half, count_places) for to in range(ntp)]
        if core == main and main > 0:
            kept = len(far_ones) // 2
            held.extend(far_ones[kept:])
            far_ones = far_ones[:kept]
        else:
            far_ones = held + far_ones
        for far_one in far_ones:
            far_one()

    held = []

    @on_main
    def _():
        for core in range(main, -1, -1):
            run_experts(core)

    with scope("final"):
        for dy in other_planes:
            d_copy(dy).wait_recv()
        on_main(lambda: whole(ret.at[1:], r_r.at[0]).wait_recv())
        on_side(lambda: whole(ret, r_r.at[0]).wait_recv())
        total = ret[0].astype(F32)
        for i in range(1, ret.shape[0]):
            total = total + ret[i].astype(F32)
        for dy in other_planes:
            total = total + dense_ref[dy - 1].astype(F32)
        own = own + unpack(total, rows)
        out_ref[...] = own[:rows].astype(BF16)
    with scope("sendwait"):
        for copy in pending:
            copy.wait_send()

        @on_main
        def _():
            whole(weights.at[0, 1:], w_s.at[0]).wait_send()
            whole(blocks.at[0, 1:], g_s.at[0]).wait_send()
            whole(ret_send.at[1:], r_s.at[0]).wait_send()

        @on_side
        def _():
            whole(weights.at[0], w_s.at[0]).wait_send()
            whole(blocks.at[0], g_s.at[0]).wait_send()
            for copy in expert_copies(c):
                copy.wait_send()


def store_kernel(out_v, c_v, n_v, m_v, out_h, c_h, n_h, m_h, sem):
    copies = [
        pltpu.make_async_copy(src, dst, sem.at[0])
        for src, dst in ((out_v, out_h), (n_v, n_h), (m_v, m_h))
    ]
    states = [pltpu.make_async_copy(c_v.at[t], c_h.at[t], sem.at[1]) for t in range(c_v.shape[0])]
    for copy in copies + states:
        copy.start()
    for copy in copies:
        copy.wait()
    pltpu.make_async_copy(c_v, c_h, sem.at[1]).wait()


def local(
    sizes,
    tokens,
    norm_gain,
    w_query,
    w_key,
    w_value,
    w_input_gate,
    w_forget_gate,
    input_bias,
    forget_bias,
    state_c,
    state_n,
    state_m,
    w_mixer_out,
    ffn_gain,
    routes,
    route_scale,
    w_expert_gate,
    w_expert_up,
    w_expert_down,
    w_dense_gate,
    w_dense_up,
    w_dense_down,
    w_branch_gate,
):
    nz, nx, nc, ntp = sizes
    rows, width = tokens.shape
    pad_rows = -(-rows // 16) * 16
    cw = width // ntp
    vmem = pl.BlockSpec(memory_space=pltpu.VMEM)
    hbm = pl.BlockSpec(memory_space=pl.ANY)
    dma = pltpu.SemaphoreType.DMA
    wide_block = block_shape(rows, pad_rows, width)
    slim_block = block_shape(rows, pad_rows, cw)
    planes = max(1, ntp - 1)
    outs = pl.pallas_call(
        functools.partial(layer_kernel, sizes),
        name="layer",
        out_shape=(
            pltpu.VMEM((rows, cw), BF16),
            pltpu.VMEM(state_c.shape, F32),
            pltpu.VMEM(state_n.shape, F32),
            pltpu.VMEM(state_m.shape[::-1], F32),
        ),
        in_specs=[hbm] * 23,
        out_specs=(vmem,) * 4,
        scratch_shapes=[
            pltpu.VMEM(tokens.shape, BF16),
            pltpu.VMEM((1, width), F32),
            pltpu.VMEM(w_input_gate.shape[::-1], BF16),
            pltpu.VMEM(w_forget_gate.shape[::-1], BF16),
            pltpu.VMEM((1, input_bias.shape[0]), F32),
            pltpu.VMEM((1, forget_bias.shape[0]), F32),
            pltpu.VMEM(state_m.shape[::-1], F32),
            pltpu.VMEM(state_n.shape, F32),
            pltpu.VMEM(w_query.shape, BF16),
            pltpu.VMEM(w_key.shape, BF16),
            pltpu.VMEM(w_value.shape, BF16),
            pltpu.VMEM(state_c.shape, F32),
            pltpu.VMEM(w_mixer_out.shape, BF16),
            pltpu.VMEM((1, width), F32),
            pltpu.VMEM(routes.shape[::-1], jnp.int32),
            pltpu.VMEM(route_scale.shape[::-1], BF16),
            pltpu.VMEM((width // 128, 128), BF16),
            pltpu.VMEM(w_dense_gate.shape, BF16),
            pltpu.VMEM(w_dense_up.shape, BF16),
            pltpu.VMEM(w_dense_down.shape, BF16),
            pltpu.VMEM((nc,) + w_expert_gate.shape[1:], BF16),
            pltpu.VMEM((nc,) + w_expert_up.shape[1:], BF16),
            pltpu.VMEM((nc,) + w_expert_down.shape[1:], BF16),
            pltpu.VMEM(wide_block, BF16),
            pltpu.VMEM((planes,) + wide_block, BF16),
            pltpu.VMEM((nz * nx, nc, 128), F32),
            pltpu.VMEM((nc, nz * nx, nc, 128), F32),
            pltpu.VMEM(wide_block, BF16),
            pltpu.VMEM((nc, nz * nx) + wide_block, BF16),
            pltpu.VMEM((nc, nz * nx * pad_rows, width), BF16),
            pltpu.VMEM((planes,) + slim_block, BF16),
            pltpu.VMEM((planes,) + slim_block, BF16),
            pltpu.VMEM((nc * ntp * nz * nx,) + slim_block, BF16),
            pltpu.VMEM((ntp * nz * nx,) + slim_block, BF16),
            dma((8,)),
            dma((planes,)),
            dma((planes,)),
            dma((1,)),
            dma((nc,)),
            dma((1,)),
            dma((nc,)),
            dma((max(1, nc - 1), 3)),
            dma((max(1, nc - 1), 3)),
            dma((planes,)),
            dma((planes,)),
            dma((1,)),
            dma((1,)),
        ],
        compiler_params=pltpu.CompilerParams(
            vmem_limit_bytes=VMEM_LIMIT, collective_id=0, has_side_effects=True
        ),
    )(
        tokens,
        norm_gain.reshape(1, width),
        w_input_gate.T,
        w_forget_gate.T,
        input_bias.reshape(1, -1),
        forget_bias.reshape(1, -1),
        state_m.T,
        state_n,
        w_query,
        w_key,
        w_value,
        state_c,
        w_mixer_out,
        ffn_gain.reshape(1, width),
        routes.T,
        route_scale.T,
        w_branch_gate.reshape(width // 128, 128),
        w_dense_gate,
        w_dense_up,
        w_dense_down,
        w_expert_gate,
        w_expert_up,
        w_expert_down,
    )
    output, new_c, new_n, new_m = pl.pallas_call(
        store_kernel,
        name="store",
        out_shape=(
            jax.ShapeDtypeStruct((rows, cw), BF16),
            jax.ShapeDtypeStruct(state_c.shape, F32),
            jax.ShapeDtypeStruct(state_n.shape, F32),
            jax.ShapeDtypeStruct(state_m.shape[::-1], F32),
        ),
        in_specs=[vmem] * 4,
        out_specs=(hbm,) * 4,
        scratch_shapes=[dma((2,))],
        compiler_params=pltpu.CompilerParams(vmem_limit_bytes=1024 * 1024),
    )(*outs)
    return (output, new_c, new_n, new_m.T)


def solution(mesh):
    n_ep, n_tp = mesh.shape["ep"], mesh.shape["tp"]
    n_core = 2 if n_ep % 2 == 0 else 1
    n_x = n_tp if n_ep % (n_core * n_tp) == 0 else 1
    sizes = (n_ep // (n_core * n_x), n_x, n_core, n_tp)
    in_specs = (
        P("ep", None),
        P(),
        P(None, "tp"),
        P(None, "tp"),
        P(None, "tp"),
        P(),
        P(),
        P(),
        P(),
        P("ep", "tp", None, None),
        P("ep", "tp", None),
        P("ep", "tp"),
        P("tp", None),
        P(),
        P("ep", None),
        P("ep", None),
        P("ep", None, "tp"),
        P("ep", None, "tp"),
        P("ep", "tp", None),
        P(None, "tp"),
        P(None, "tp"),
        P("tp", None),
        P(),
    )
    out_specs = (P("ep", "tp"), P("ep", "tp", None, None), P("ep", "tp", None), P("ep", "tp"))
    return jax.shard_map(
        functools.partial(local, sizes),
        mesh=mesh,
        in_specs=in_specs,
        out_specs=out_specs,
        check_vma=False,
    )
```
